128 devices in a mesh: rep: 16 (over z, x), fs: 4 (over y), tp: 2 (over core).
Axes of the slice: x: 4, y: 4, z: 4, core: 2. Of those that a mesh axis runs over, the one named last changes fastest.
Arguments:
- inputs: bfloat16 [64, 768, 2048], P(('rep', 'fs'), 'tp'), may hold values from -6 to 6
- pre_gate: bfloat16 [64, 768, 2816], P(('rep', 'fs'), None, 'tp'), may hold values from -6 to 6
- pre_up: bfloat16 [64, 768, 2816], P(('rep', 'fs'), None, 'tp'), may hold values from -6 to 6
- cotangent: bfloat16 [64, 768, 2816], P(('rep', 'fs'), None, 'tp'), may hold values from -16 to 16
- w_gate: bfloat16 [2048, 2816], P('fs', 'tp'), may hold values from -0.125 to 0.125
- w_up: bfloat16 [2048, 2816], P('fs', 'tp'), may hold values from -0.125 to 0.125
- taps_gate: bfloat16 [3, 2816], replicated, may hold values from -3 to 3
- taps_up: bfloat16 [3, 2816], replicated, may hold values from -3 to 3
Outputs:
- grad_inputs: bfloat16 [64, 768, 2048], P(('rep', 'fs'), 'tp')
- grad_w_gate: float32 [2048, 2816], P('fs', 'tp')
- grad_w_up: float32 [2048, 2816], P('fs', 'tp')
- grad_taps_gate: float32 [3, 2816], replicated
- grad_taps_up: float32 [3, 2816], replicated
The draws below stay inside these ranges and needn't reach their ends.
All inputs are finite; a program needn't handle non-finite values.
Results may differ from the reference program's by a relative error of at most 0.0059.
Values may be sent and summed in bfloat16 or wider, within the bound.
A program may use at most 192 MiB of HBM per device.

```python
import jax
import jax.numpy as jnp
from jax import lax

D = 2048
F = 2816
TAPS = 3
LEN = 768
SEQS = 64
TOKENS = 49152
N_TP = 2


def raised(entries, own_key, source, target, parts, factor):
    def block_of(axis_at):
        return (jnp.arange(entries.shape[axis_at]) // (entries.shape[axis_at] // parts)).reshape((-1,) + (1,) * (entries.ndim - 1 - axis_at))

    first = jax.random.permutation(own_key, parts)[block_of(target)]
    other_side = (block_of(target) + parts // 2) % parts
    return jnp.where((block_of(source) == first) | (block_of(source) == other_side), factor * entries, entries)


def levels(own_key, shape, cuts, low, top_value):
    def one(axis_at, shards_of):
        heights = jax.random.uniform(jax.random.fold_in(jax.random.fold_in(own_key, 6), axis_at), (shards_of,), jnp.float32, low / len(cuts), top_value / len(cuts))
        return jnp.repeat(jnp.exp(heights), shape[axis_at] // shards_of).reshape((-1,) + (1,) * (len(shape) - axis_at - 1))

    gain = one(*cuts[0])
    for cut in cuts[1:]:
        gain = gain * one(*cut)
    return gain


def gaussian(own_key, dims, spread, most, split=(), kind=jnp.bfloat16):
    result = spread * jax.random.normal(own_key, dims, jnp.float32)
    if split:
        result = result * levels(own_key, dims, split, -0.22, 0.18)
    return jnp.clip(result, -most, most).astype(kind)


def noise_with(own_key, shape, spread, limit, split, heavy, held_as=jnp.bfloat16):
    entries = spread * jax.random.normal(own_key, shape, jnp.float32)
    if split:
        entries = entries * levels(own_key, shape, split, -0.22, 0.18)
    return jnp.clip(raised(entries, jax.random.fold_in(own_key, 3), *heavy), -limit, limit).astype(held_as)


def setup_inputs(seed: int = 0) -> dict:
    streams_of = jax.random.split(jax.random.key(seed), 9)
    inputs = gaussian(streams_of[0], (SEQS, LEN, D), 1.0, 6.0, ((0, 64), (1, 2)))
    pre_gate = gaussian(streams_of[1], (SEQS, LEN, F), 1.0, 6.0, ((0, 64), (2, 2)))
    pre_up = gaussian(streams_of[2], (SEQS, LEN, F), 1.0, 6.0, ((0, 64), (2, 2)))
    cotangent = noise_with(streams_of[3], (SEQS, LEN, F), 1.0, 16.0, ((0, 64), (2, 2)), (0, 2, 64, 4.0))
    w_gate = gaussian(streams_of[4], (D, F), D ** -0.5, 0.125, ((0, 4), (1, 2)))
    w_up = gaussian(streams_of[5], (D, F), D ** -0.5, 0.125, ((0, 4), (1, 2)))
    taps_gate = gaussian(streams_of[6], (TAPS, F), 0.6, 3.0)
    taps_up = gaussian(streams_of[7], (TAPS, F), 0.6, 3.0)
    return dict(inputs=inputs, pre_gate=pre_gate, pre_up=pre_up, cotangent=cotangent, w_gate=w_gate, w_up=w_up, taps_gate=taps_gate, taps_up=taps_up)


def causal_mix(signal, kernel):
    length = signal.shape[0]
    padded = jnp.pad(signal, ((2, 0), (0, 0)))
    return kernel[0] * padded[0:length] + kernel[1] * padded[1:length + 1] + kernel[2] * padded[2:length + 2]

def gated_hidden(gate_pre, up_pre, kernel_gate, kernel_up):
    return jax.nn.gelu(causal_mix(gate_pre, kernel_gate)) * causal_mix(up_pre, kernel_up)

def reference(inputs, pre_gate, pre_up, cotangent, w_gate, w_up, taps_gate, taps_up):
    kernel_gate = taps_gate.astype(jnp.float32)
    kernel_up = taps_up.astype(jnp.float32)
    block = F // N_TP

    def one_sequence(totals, item):
        rows, gate_seq, up_seq, back_seq = item
        _, pullback = jax.vjp(gated_hidden, gate_seq.astype(jnp.float32), up_seq.astype(jnp.float32), kernel_gate, kernel_up)
        back_gate, back_up, tap_gate, tap_up = pullback(back_seq.astype(jnp.float32))
        grad_gate = back_gate.astype(jnp.bfloat16)
        grad_up = back_up.astype(jnp.bfloat16)
        summed = jnp.zeros((rows.shape[0], rows.shape[1]), jnp.float32)
        for index in range(N_TP):
            lower = index * block
            partial_value = jnp.dot(grad_gate[:, lower:lower + block], w_gate[:, lower:lower + block].T, preferred_element_type=jnp.float32)
            partial_value = partial_value + jnp.dot(grad_up[:, lower:lower + block], w_up[:, lower:lower + block].T, preferred_element_type=jnp.float32)
            rounded = lax.optimization_barrier(partial_value.astype(jnp.bfloat16))
            summed = summed + rounded.astype(jnp.float32)
        new_totals = (totals[0] + jnp.dot(rows.T, grad_gate, preferred_element_type=jnp.float32), totals[1] + jnp.dot(rows.T, grad_up, preferred_element_type=jnp.float32), totals[2] + tap_gate, totals[3] + tap_up)
        return (new_totals, summed.astype(jnp.bfloat16))
    start = (jnp.zeros((D, F), jnp.float32), jnp.zeros((D, F), jnp.float32), jnp.zeros((TAPS, F), jnp.float32), jnp.zeros((TAPS, F), jnp.float32))
    totals, grad_inputs = lax.scan(one_sequence, start, (inputs, pre_gate, pre_up, cotangent))
    factor = float(TOKENS) ** (-0.5)
    return (grad_inputs, totals[0] * factor, totals[1] * factor, totals[2] * factor, totals[3] * factor)
```

```python
import functools

import jax
import jax.numpy as jnp
from jax import lax
from jax.experimental import pallas as pl
from jax.experimental.pallas import tpu as pltpu
from jax.sharding import PartitionSpec as P

MESH = pl.DeviceIdType.MESH
LEN = 768
COLS = 1408
WIDTH = 2048
TOKENS = 49152
SPLITS = ((0, 640), (640, 768))
CHUNK = 64
PAD = 16
HALF = LEN // 2
ROOT = 0.7978845608028654
CUBIC = 0.044715
bf16, f32 = jnp.bfloat16, jnp.float32


def wrap(value, n=4):
    return lax.rem(value + 2 * n, n)


def mult(value, n):
    return pl.multiple_of(value, n)


def kernel(
    x_hbm, pg_hbm, pu_hbm, ct_hbm, wg_hbm, wu_hbm, tg_ref, tu_ref,
    gi_out, ag_out, tog_ref, tou_ref,
    pg, pu, ct, xs, xt, wall, buf0, buf1, own, acc1, two0, two1, acc2,
    out3_0, out3_1, in3_0, in3_1, ag, taps, tfin, gsend, gown, grecv,
    loc, xsem, w1s, w1r, w2s, w2r, p1s, p1r, p2s, p2r, p3s, p3r,
    a1s, a1r, a2s, a2r, a3s, a3r, tss, tsr, gss, gsr,
):
    rep, y, c = lax.axis_index("rep"), lax.axis_index("fs"), lax.axis_index("tp")
    z, x = rep // 4, lax.rem(rep, 4)
    first, second = (x, z), (z, x)
    bufs, twos = (buf0, buf1), (two0, two1)
    outs3, ins3 = (out3_0, out3_1), (in3_0, in3_1)

    def dev(dx=0, dz=0, dy=0, dc=0):
        return (wrap(z + dz) * 4 + wrap(x + dx), wrap(y + dy), wrap(c + dc, 2))

    def first_dev(p, d):
        return dev(dx=d) if p == 0 else dev(dz=d)

    def second_dev(p, d):
        return dev(dz=d) if p == 0 else dev(dx=d)

    def remote(src, dst, send, recv, where):
        return pltpu.make_async_remote_copy(
            src_ref=src, dst_ref=dst, send_sem=send, recv_sem=recv, device_id=where, device_id_type=MESH
        )

    started = []

    def send(src, dst, send_sem, recv_sem, where):
        copy = remote(src, dst, send_sem, recv_sem, where)
        copy.start()
        started.append(copy)
        return copy

    local = []

    def load(src, dst):
        copy = pltpu.make_async_copy(src, dst, loc.at[len(local)])
        copy.start()
        local.append(copy)
        return copy

    pre = []
    for at, width in SPLITS:
        cols = pl.ds(at, width)
        pre.append(
            [load(h.at[0, :, cols], v.at[pl.ds(PAD, LEN), cols]) for h, v in ((pg_hbm, pg), (pu_hbm, pu), (ct_hbm, ct))]
        )
    mine = pl.ds(mult(c * HALF, HALF), HALF)
    x_local = load(x_hbm.at[0], xs.at[mine])
    w_local = [load(h, wall.at[g, y]) for g, h in enumerate((wg_hbm, wu_hbm))]
    pg[0:PAD, :] = jnp.zeros((PAD, COLS), bf16)
    pu[0:PAD, :] = jnp.zeros((PAD, COLS), bf16)

    peers = [dev(dx=d) for d in (1, 2, 3)] + [dev(dz=d) for d in (1, 2, 3)]
    peers += [dev(dy=d) for d in (1, 2, 3)] + [dev(dc=1)]
    barrier = pltpu.get_barrier_semaphore()
    for peer in peers:
        pl.semaphore_signal(barrier, inc=1, device_id=peer, device_id_type=MESH)
    pl.semaphore_wait(barrier, len(peers))

    x_send = send(x_hbm.at[0], xs.at[mine], xsem.at[0], xsem.at[1], dev(dc=1))
    hbm_w = (wg_hbm, wu_hbm)

    def w_rows(half):
        return pl.ds(half * 256, 256)

    for order in range(2):
        for g in range(2):
            for way in range(2):
                half = order if way == 0 else 1 - order
                index = way * 4 + order * 2 + g
                send(
                    hbm_w[g].at[w_rows(half)], wall.at[g, y, w_rows(half)], w1s.at[index], w1r.at[index],
                    dev(dy=1 if way == 0 else -1),
                )

    def w_arrived(way, order, g):
        half = order if way == 0 else 1 - order
        index = way * 4 + order * 2 + g
        place = wall.at[g, wrap(y - 1 if way == 0 else y + 1), w_rows(half)]
        remote(place, place, w1s.at[index], w1r.at[index], dev(dy=1)).wait_recv()

    def w_forward(g):
        for way in range(2):
            w_arrived(way, 0, g)
            place = wall.at[g, wrap(y - 1 if way == 0 else y + 1), w_rows(way)]
            send(place, place, w2s.at[way * 2 + g], w2r.at[way * 2 + g], dev(dy=1 if way == 0 else -1))

    def w_far_arrived(way, g):
        place = wall.at[g, wrap(y + 2), w_rows(way)]
        remote(place, place, w2s.at[way * 2 + g], w2r.at[way * 2 + g], dev(dy=1)).wait_recv()

    def elementwise(k):
        at, width = SPLITS[k]

        def column(b, _):
            col = mult(at + b * 128, 128)
            cols = pl.ds(col, 128)
            shared = pl.ds(mult(c * COLS + col, 128), 128)
            kg = tg_ref[:, shared].astype(f32)
            ku = tu_ref[:, shared].astype(f32)
            kg = [kg[j : j + 1] for j in range(3)]
            ku = [ku[j : j + 1] for j in range(3)]

            def rows(i, carry):
                next_g, next_u, sums = carry
                r = mult(LEN - CHUNK - i * CHUNK, CHUNK)
                span, here = pl.ds(r, CHUNK + PAD), pl.ds(r + PAD, CHUNK)
                eg = pg[span, cols].astype(f32)[8:]
                eu = pu[span, cols].astype(f32)[8:]
                co = ct[here, cols].astype(f32)
                sg = [pltpu.roll(eg, 2, 0)[8:], pltpu.roll(eg, 1, 0)[8:], eg[8:]]
                su = [pltpu.roll(eu, 2, 0)[8:], pltpu.roll(eu, 1, 0)[8:], eu[8:]]
                v = kg[0] * sg[0] + kg[1] * sg[1] + kg[2] * sg[2]
                m = ku[0] * su[0] + ku[1] * su[1] + ku[2] * su[2]
                v2 = v * v
                t = jnp.tanh(v * (ROOT + (ROOT * CUBIC) * v2))
                h = 0.5 + 0.5 * t
                slope = h * (1.0 + v * (1.0 - t) * (ROOT + (3.0 * ROOT * CUBIC) * v2))
                bg = co * m * slope
                bu = co * (v * h)
                new = tuple(
                    s + (back * moved).reshape(CHUNK // 8, 8, 128).sum(0)
                    for s, (back, moved) in zip(sums, [(bg, q) for q in sg] + [(bu, q) for q in su])
                )
                for ref, back, after, taps_of in ((pg, bg, next_g, kg), (pu, bu, next_u, ku)):
                    whole = jnp.concatenate([back, after], axis=0)
                    one = pltpu.roll(whole, CHUNK + 7, 0)[:CHUNK]
                    two = pltpu.roll(whole, CHUNK + 6, 0)[:CHUNK]
                    ref[here, cols] = (taps_of[2] * back + taps_of[1] * one + taps_of[0] * two).astype(bf16)
                return bg[:8], bu[:8], new

            zero = jnp.zeros((8, 128), f32)
            _, _, sums = lax.fori_loop(0, LEN // CHUNK, rows, (zero, zero, (zero,) * 6))
            rows8 = [jnp.sum(s, axis=0, keepdims=True) for s in sums]
            taps[0, x, :, cols] = jnp.concatenate(rows8 + [jnp.zeros((2, 128), f32)], axis=0)
            return 0

        lax.fori_loop(0, width // 128, column, 0)

    grads = (pg, pu)

    def own_rows(p, s):
        parts = []
        for yb in range(4):
            chunk = wrap(first[p] - 1 - s) if yb < 2 else wrap(first[p] + 1 + s)
            parts.append(xt[pl.ds(mult(yb * 512 + chunk * 128, 128), 128), :])
        return jnp.concatenate(parts, axis=0)

    def product(p, k, s):
        at, width = SPLITS[k]
        right = grads[p][PAD : PAD + LEN, at : at + width]
        return jnp.dot(own_rows(p, s), right, preferred_element_type=f32).reshape(4, 128, width)

    def p1_index(k, p, way, s):
        return ((k * 2 + p) * 2 + way) * 3 + s

    def p1_copy(k, p, way, s):
        pair = pl.ds(way * 2, 2)
        index = p1_index(k, p, way, s)
        return (
            bufs[k].at[p, s, pair], bufs[k].at[p, s + 1, pair], p1s.at[index], p1r.at[index],
            first_dev(p, 1 if way == 0 else -1),
        )

    def step0(k):
        for p in range(2):
            bufs[k][p, 0] = product(p, k, 0).astype(bf16)
            for way in range(2):
                send(*p1_copy(k, p, way, 0))

    def step1(k, s):
        at, width = SPLITS[k]
        for p in range(2):
            own[p, :, :, 0:width] = product(p, k, s)
        for p in range(2):
            for way in range(2):
                remote(*p1_copy(k, p, way, s - 1)).wait_recv()

            def add(yb, _):
                total = bufs[k][p, s, yb].astype(f32) + own[p, yb, :, 0:width]
                if s < 3:
                    bufs[k][p, s, yb] = total.astype(bf16)
                else:
                    acc1[p, yb, :, at : at + width] = total
                return 0

            lax.fori_loop(0, 4, add, 0)
            if s < 3:
                for way in range(2):
                    send(*p1_copy(k, p, way, s))

    def p2_copy(k, p, way, s):
        pair = pl.ds(way * 2, 2)
        index = p1_index(k, p, way, s)
        return (
            twos[k].at[p, s, pair], twos[k].at[p, s + 1, pair], p2s.at[index], p2r.at[index],
            second_dev(p, 1 if way == 0 else -1),
        )

    def step2(k, s):
        at, width = SPLITS[k]
        for p in range(2):
            if s > 0:
                for way in range(2):
                    remote(*p2_copy(k, p, way, s - 1)).wait_recv()

            def add(yb, _):
                move = (1 - 2 * (yb // 2)) * (1 + s)
                chunk = wrap(second[p] - move)
                total = acc1[p, yb, pl.ds(mult(chunk * 32, 32), 32), at : at + width]
                if s > 0:
                    total = total + twos[k][p, s, yb].astype(f32)
                if s < 3:
                    twos[k][p, s, yb] = total.astype(bf16)
                else:
                    acc2[p, yb, :, at : at + width] = total
                return 0

            lax.fori_loop(0, 4, add, 0)
            if s < 3:
                for way in range(2):
                    send(*p2_copy(k, p, way, s))

    def p3_copy(k, p, d):
        index = (k * 2 + p) * 3 + d - 1
        return outs3[k].at[p, d - 1], ins3[k].at[p, d - 1], p3s.at[index], p3r.at[index], dev(dy=d)

    def p3_send(k):
        at, width = SPLITS[k]
        for p in range(2):
            for d in (1, 3, 2):
                outs3[k][p, d - 1] = acc2[p, wrap(y + d), :, at : at + width].astype(bf16)
                send(*p3_copy(k, p, d))

    def block(p, d_first, d_second, skip=0, rows=32):
        start = wrap(first[p] + d_first) * 128 + wrap(second[p] + d_second) * 32 + skip
        return ag.at[p, pl.ds(mult(start, 16), rows)]

    def p3_finish(k, p):
        at, width = SPLITS[k]
        total = acc2[p, y, :, at : at + width]
        for d in (1, 3, 2):
            remote(*p3_copy(k, p, d)).wait_recv()
            total = total + ins3[k][p, d - 1].astype(f32)
        start = mult(first[p] * 128 + second[p] * 32, 32)
        ag[p, pl.ds(start, 32), at : at + width] = total.astype(bf16)

    def a1_start(p):
        for d in (1, 3, 2):
            index = p * 3 + d - 1
            place = block(p, 0, 0)
            send(place, place, a1s.at[index], a1r.at[index], second_dev(p, d))

    def a1_wait(p, d):
        index = p * 3 + d - 1
        place = block(p, 0, -d)
        remote(place, place, a1s.at[index], a1r.at[index], second_dev(p, d)).wait_recv()

    def a2_start(p, d):
        for way in range(2):
            index = (p * 2 + way) * 4 + d
            place = block(p, 0, -d)
            send(place, place, a2s.at[index], a2r.at[index], first_dev(p, 1 if way == 0 else -1))

    def a2_pass_on(p, d):
        for way in range(2):
            index = (p * 2 + way) * 4 + d
            from_ = -1 if way == 0 else 1
            place = block(p, from_, -d)
            remote(place, place, a2s.at[index], a2r.at[index], first_dev(p, 1)).wait_recv()
            part = block(p, from_, -d, 16 * way, 16)
            send(part, part, a3s.at[index], a3r.at[index], first_dev(p, -from_))

    def a3_wait(p, d):
        for way in range(2):
            index = (p * 2 + way) * 4 + d
            place = block(p, 2, -d, 16 * way, 16)
            remote(place, place, a3s.at[index], a3r.at[index], first_dev(p, 1)).wait_recv()

    coords = (x, z, y)

    def tap_dev(stage, d):
        return dev(dx=d) if stage == 0 else dev(dz=d) if stage == 1 else dev(dy=d)

    def tap_send(stage):
        place = taps.at[stage, coords[stage]]
        for d in (1, 2, 3):
            index = stage * 3 + d - 1
            send(place, place, tss.at[index], tsr.at[index], tap_dev(stage, d))

    def tap_sum(stage):
        for d in (1, 2, 3):
            index = stage * 3 + d - 1
            place = taps.at[stage, wrap(coords[stage] - d)]
            remote(place, place, tss.at[index], tsr.at[index], tap_dev(stage, d)).wait_recv()
        total = taps[stage, 0] + taps[stage, 1] + taps[stage, 2] + taps[stage, 3]
        if stage < 2:
            taps[stage + 1, coords[stage + 1]] = total
            tap_send(stage + 1)
        else:
            tfin[c] = total * (float(TOKENS) ** -0.5)
            send(tfin.at[c], tfin.at[c], tss.at[9], tsr.at[9], dev(dc=1))

    def tap_end():
        other = tfin.at[wrap(c + 1, 2)]
        remote(other, other, tss.at[9], tsr.at[9], dev(dc=1)).wait_recv()
        for side in range(2):
            cols = slice(side * COLS, side * COLS + COLS)
            tog_ref[:, cols] = tfin[side, 0:3]
            tou_ref[:, cols] = tfin[side, 3:6]

    def project(unit, d, half):
        shard = wrap(y + d)

        def side(which, _):
            to_partner = 1 - which
            row = mult(PAD + wrap(c + to_partner, 2) * HALF, 16)
            value = lax.dot_general(
                pg[pl.ds(row, HALF), :], wall[0, shard, half * 256 : half * 256 + 256, :],
                (((1,), (1,)), ((), ())), preferred_element_type=f32,
            )
            value = value + lax.dot_general(
                pu[pl.ds(row, HALF), :], wall[1, shard, half * 256 : half * 256 + 256, :],
                (((1,), (1,)), ((), ())), preferred_element_type=f32,
            )
            gsend[which, unit] = value.astype(bf16)
            return 0

        lax.fori_loop(0, 2, side, 0)
        send(gsend.at[0, unit], grecv.at[unit], gss.at[unit], gsr.at[unit], dev(dc=1))

    out_copies = []

    def combine(unit, d, half):
        remote(gsend.at[0, unit], grecv.at[unit], gss.at[unit], gsr.at[unit], dev(dc=1)).wait_recv()
        gown[unit] = (gsend[1, unit].astype(f32) + grecv[unit].astype(f32)).astype(bf16)
        col = mult(wrap(y + d) * 512 + half * 256, 256)
        out_copies.append(load(gown.at[unit], gi_out.at[:, pl.ds(col, 256)]))

    for copy in pre[0]:
        copy.wait()
    elementwise(0)
    x_local.wait()
    other = xs.at[pl.ds(mult(wrap(c + 1, 2) * HALF, HALF), HALF)]
    remote(other, other, xsem.at[0], xsem.at[1], dev(dc=1)).wait_recv()

    def turn(b, _):
        at = mult(b * 128, 128)
        xt[pl.ds(at, 128), :] = xs[:, pl.ds(at, 128)].T
        return 0

    lax.fori_loop(0, WIDTH // 128, turn, 0)
    step0(0)
    for copy in pre[1]:
        copy.wait()
    elementwise(1)
    step0(1)
    tap_send(0)
    step1(0, 1)
    step1(1, 1)
    tap_sum(0)
    for copy in w_local:
        copy.wait()
    project(0, 0, 0)
    step1(0, 2)
    project(1, 0, 1)
    step1(1, 2)
    tap_sum(1)
    w_forward(0)
    combine(0, 0, 0)
    combine(1, 0, 1)
    step1(0, 3)
    step2(0, 0)
    w_arrived(0, 0, 1)
    w_arrived(1, 0, 1)
    project(2, -1, 0)
    step1(1, 3)
    step2(1, 0)
    tap_sum(2)
    project(3, 1, 1)
    step2(0, 1)
    step2(1, 1)
    combine(2, -1, 0)
    combine(3, 1, 1)
    step2(0, 2)
    step2(1, 2)
    for g in range(2):
        w_arrived(0, 1, g)
        w_arrived(1, 1, g)
    project(4, -1, 1)
    step2(0, 3)
    p3_send(0)
    step2(1, 3)
    p3_send(1)
    for way in range(2):
        place = wall.at[1, wrap(y - 1 if way == 0 else y + 1), w_rows(way)]
        send(place, place, w2s.at[way * 2 + 1], w2r.at[way * 2 + 1], dev(dy=1 if way == 0 else -1))
    project(5, 1, 0)
    for p in range(2):
        p3_finish(0, p)
    for p in range(2):
        p3_finish(1, p)
        a1_start(p)
        a2_start(p, 0)
    for d in (1, 3, 2):
        for p in range(2):
            a1_wait(p, d)
            a2_start(p, d)
    combine(4, -1, 1)
    combine(5, 1, 0)
    tap_end()
    for d in (0, 1, 3, 2):
        for p in range(2):
            a2_pass_on(p, d)
    for way in range(2):
        for g in range(2):
            w_far_arrived(way, g)
    project(6, 2, 0)
    project(7, 2, 1)
    for d in (0, 1, 3, 2):
        for p in range(2):
            a3_wait(p, d)
    for p in range(2):
        out_copies.append(load(ag.at[p], ag_out.at[p]))
    combine(6, 2, 0)
    combine(7, 2, 1)
    for copy in started:
        copy.wait_send()
    for copy in out_copies:
        copy.wait()


def per_device(inputs, pre_gate, pre_up, cotangent, w_gate, w_up, taps_gate, taps_up):
    any_ = pl.BlockSpec(memory_space=pl.ANY)
    vmem = pl.BlockSpec(memory_space=pltpu.VMEM)
    dma = pltpu.SemaphoreType.DMA
    widths = [width for _, width in SPLITS]
    scratch = (
        [pltpu.VMEM((PAD + LEN, COLS), bf16)] * 3
        + [pltpu.VMEM((LEN, WIDTH), bf16), pltpu.VMEM((WIDTH, LEN), bf16), pltpu.VMEM((2, 4, 512, COLS), bf16)]
        + [pltpu.VMEM((2, 4, 4, 128, width), bf16) for width in widths]
        + [pltpu.VMEM((2, 4, 128, max(widths)), f32), pltpu.VMEM((2, 4, 128, COLS), f32)]
        + [pltpu.VMEM((2, 4, 4, 32, width), bf16) for width in widths]
        + [pltpu.VMEM((2, 4, 32, COLS), f32)]
        + [pltpu.VMEM((2, 3, 32, width), bf16) for width in widths] * 2
        + [pltpu.VMEM((2, 512, COLS), bf16), pltpu.VMEM((3, 4, 8, COLS), f32), pltpu.VMEM((2, 8, COLS), f32)]
        + [pltpu.VMEM((2, 8, HALF, 256), bf16), pltpu.VMEM((8, HALF, 256), bf16), pltpu.VMEM((8, HALF, 256), bf16)]
        + [dma((32,)), dma((2,)), dma((8,)), dma((8,)), dma((4,)), dma((4,))]
        + [dma((24,))] * 4
        + [dma((12,))] * 2
        + [dma((6,))] * 2
        + [dma((16,))] * 4
        + [dma((10,))] * 2
        + [dma((8,))] * 2
    )
    grad_inputs, sums, tap_gate, tap_up = pl.pallas_call(
        kernel,
        out_shape=(
            jax.ShapeDtypeStruct((HALF, WIDTH), bf16),
            jax.ShapeDtypeStruct((2, 512, COLS), bf16),
            jax.ShapeDtypeStruct((3, 2 * COLS), f32),
            jax.ShapeDtypeStruct((3, 2 * COLS), f32),
        ),
        in_specs=[any_] * 6 + [vmem] * 2,
        out_specs=(any_, any_, vmem, vmem),
        scratch_shapes=scratch,
        compiler_params=pltpu.CompilerParams(
            collective_id=0, has_side_effects=True, vmem_limit_bytes=67043328
        ),
    )(inputs, pre_gate, pre_up, cotangent, w_gate, w_up, taps_gate, taps_up)
    factor = float(TOKENS) ** -0.5
    return (
        grad_inputs[None],
        sums[0].astype(f32) * factor,
        sums[1].astype(f32) * factor,
        tap_gate,
        tap_up,
    )


def solution(mesh):
    placed = (
        P(("rep", "fs"), "tp", None),
        P(("rep", "fs"), None, "tp"),
        P(("rep", "fs"), None, "tp"),
        P(("rep", "fs"), None, "tp"),
        P("fs", "tp"),
        P("fs", "tp"),
        P(),
        P(),
    )
    return jax.shard_map(
        per_device,
        mesh=mesh,
        in_specs=placed,
        out_specs=(P(("rep", "fs"), "tp", None), P("fs", "tp"), P("fs", "tp"), P(), P()),
        check_vma=False,
    )
```

```python
import functools

import jax
import jax.numpy as jnp
from jax import lax
from jax.experimental import pallas as pl
from jax.experimental.pallas import tpu as pltpu
from jax.sharding import PartitionSpec as P

MESH = pl.DeviceIdType.MESH
LEN = 768
COLS = 1408
WIDTH = 2048
TOKENS = 49152
SPLITS = ((0, 256), (256, 512), (768, 640))
CHUNK = 64
PAD = 16
STRIPE = 32
FAR = ((0, 128), (128, 64), (192, 64))
GROUPS = ((0, 768), (768, 640))
HALF = LEN // 2
ROOT = 0.7978845608028654
CUBIC = 0.044715
bf16, f32 = jnp.bfloat16, jnp.float32


def wrap(value, n=4):
    return lax.rem(value + 2 * n, n)


def mult(value, n):
    return pl.multiple_of(value, n)


def kernel(
    x_hbm, pg_hbm, pu_hbm, ct_hbm, wg_hbm, wu_hbm, tg_hbm, tu_hbm,
    gi_out, ag_out, tap_out,
    pg, pu, ct, xs, xt, wall, buf0, buf1, buf2, own, acc1, two0, two1, two2, acc2,
    out3_0, out3_1, out3_2, in3_0, in3_1, in3_2, ag, taps, tfin, gsend, gown, grecv, tg_ref, tu_ref,
    loc, osem, xsem, ws, w0r, w1r, w2r, w3r, w4r, p1s, p1r, p2s, p2r, p3s, p3r,
    a1s, a1r, a2s, a2r, a3s, a3r, tss, tsr, gss, gsr,
):
    rep, y, c = lax.axis_index("rep"), lax.axis_index("fs"), lax.axis_index("tp")
    z, x = rep // 4, lax.rem(rep, 4)
    first, second = (x, z), (z, x)
    bufs, twos = (buf0, buf1, buf2), (two0, two1, two2)
    outs3, ins3 = (out3_0, out3_1, out3_2), (in3_0, in3_1, in3_2)

    def dev(dx=0, dz=0, dy=0, dc=0):
        return (wrap(z + dz) * 4 + wrap(x + dx), wrap(y + dy), wrap(c + dc, 2))

    def first_dev(p, d):
        return dev(dx=d) if p == 0 else dev(dz=d)

    def second_dev(p, d):
        return dev(dz=d) if p == 0 else dev(dx=d)

    def remote(src, dst, send, recv, where):
        return pltpu.make_async_remote_copy(
            src_ref=src, dst_ref=dst, send_sem=send, recv_sem=recv, device_id=where, device_id_type=MESH
        )

    def send(src, dst, send_sem, recv_sem, where):
        remote(src, dst, send_sem, recv_sem, where).start()

    def received(place, sem):
        remote(place, place, sem, sem, dev(dc=1)).wait_recv()

    def sent(place, sem):
        remote(place, place, sem, sem, dev(dc=1)).wait_send()

    local = []

    def load(src, dst):
        copy = pltpu.make_async_copy(src, dst, loc.at[len(local)])
        copy.start()
        local.append(copy)
        return copy

    tap_loads = [load(tg_hbm, tg_ref), load(tu_hbm, tu_ref)]
    pre = []
    for at, width in SPLITS:
        cols = pl.ds(at, width)
        pre.append(
            [load(h.at[0, :, cols], v.at[pl.ds(PAD, LEN), cols]) for h, v in ((pg_hbm, pg), (pu_hbm, pu), (ct_hbm, ct))]
        )
    mine = pl.ds(mult(c * HALF, HALF), HALF)
    x_local = load(x_hbm.at[0], xs.at[mine])
    w_local = [load(h, wall.at[g, y]) for g, h in enumerate((wg_hbm, wu_hbm))]
    pg[0:PAD, :] = jnp.zeros((PAD, COLS), bf16)
    pu[0:PAD, :] = jnp.zeros((PAD, COLS), bf16)

    peers = [dev(dx=d) for d in (1, 2, 3)] + [dev(dz=d) for d in (1, 2, 3)]
    peers += [dev(dy=d) for d in (1, 2, 3)] + [dev(dc=1)]
    barrier = pltpu.get_barrier_semaphore()
    for peer in peers:
        pl.semaphore_signal(barrier, inc=1, device_id=peer, device_id_type=MESH)
    pl.semaphore_wait(barrier, len(peers))

    send(x_hbm.at[0], xs.at[mine], xsem.at[0], xsem.at[1], dev(dc=1))
    ways = ((-1, x, 0, 512 - 4 * STRIPE), (1, z, 256, 0))

    def ring_dev(way, d):
        return dev(dx=d) if way == 0 else dev(dz=d)

    def stripe(way, d):
        source, at, _, base = ways[way]
        return wrap(y + source), pl.ds(mult(base + wrap(at + d) * STRIPE, STRIPE), STRIPE)

    def passed(way):
        source, _, start, _ = ways[way]
        return wrap(y + source), pl.ds(start, 256)

    def rest(way):
        source = ways[way][0]
        return wrap(y + source), pl.ds(256 if way == 0 else 4 * STRIPE, 256 - 4 * STRIPE)

    for level, rows_of in enumerate((lambda way: stripe(way, 0), passed, rest)):
        for g, h in enumerate((wg_hbm, wu_hbm)):
            for way in range(2):
                rows = rows_of(way)[1]
                sem = w0r.at[way] if level == 0 else w1r.at[way * 2 + level - 1]
                send(h.at[rows], wall.at[g, y, rows], ws.at[0], sem, dev(dy=-ways[way][0]))

    def stripe_start():
        for way in range(2):
            shard, rows = stripe(way, 0)
            place = wall.at[:, shard, rows]
            received(place, w0r.at[way])
            for side, d in enumerate((1, -1)):
                send(place, place, ws.at[1], w3r.at[way * 2 + side], ring_dev(way, d))

    def stripe_pass():
        for way in range(2):
            for side, d in enumerate((1, -1)):
                shard, rows = stripe(way, -d)
                received(wall.at[:, shard, rows], w3r.at[way * 2 + side])
                place = wall.at[side, shard, rows]
                send(place, place, ws.at[2], w4r.at[way * 2 + side], ring_dev(way, d))

    def stripe_end():
        for way in range(2):
            shard, rows = stripe(way, 2)
            for side in range(2):
                received(wall.at[side, shard, rows], w4r.at[way * 2 + side])

    def w_arrived(way, level):
        shard, rows = (passed, rest)[level](way)
        received(wall.at[:, shard, rows], w1r.at[way * 2 + level])

    def w_forward(piece):
        at, count = FAR[piece]
        for way in range(2):
            place = wall.at[:, wrap(y + ways[way][0]), pl.ds(way * 256 + at, count)]
            send(place, place, ws.at[3], w2r.at[way * len(FAR) + piece], dev(dy=-ways[way][0]))

    def w_far_arrived(piece):
        at, count = FAR[piece]
        for way in range(2):
            received(wall.at[:, wrap(y + 2), pl.ds(way * 256 + at, count)], w2r.at[way * len(FAR) + piece])

    def elementwise(k, low, high):
        at = SPLITS[k][0]

        def column(b, _):
            col = mult(at + b * 128, 128)
            cols = pl.ds(col, 128)
            shared = pl.ds(mult(c * COLS + col, 128), 128)
            kg = tg_ref[:, shared].astype(f32)
            ku = tu_ref[:, shared].astype(f32)
            kg = [kg[j : j + 1] for j in range(3)]
            ku = [ku[j : j + 1] for j in range(3)]

            def rows(i, carry):
                next_g, next_u, sums = carry
                r = mult(LEN - CHUNK - i * CHUNK, CHUNK)
                span, here = pl.ds(r, CHUNK + PAD), pl.ds(r + PAD, CHUNK)
                eg = pg[span, cols].astype(f32)[8:]
                eu = pu[span, cols].astype(f32)[8:]
                co = ct[here, cols].astype(f32)
                sg = [pltpu.roll(eg, 2, 0)[8:], pltpu.roll(eg, 1, 0)[8:], eg[8:]]
                su = [pltpu.roll(eu, 2, 0)[8:], pltpu.roll(eu, 1, 0)[8:], eu[8:]]
                v = kg[0] * sg[0] + kg[1] * sg[1] + kg[2] * sg[2]
                m = ku[0] * su[0] + ku[1] * su[1] + ku[2] * su[2]
                v2 = v * v
                t = jnp.tanh(v * (ROOT + (ROOT * CUBIC) * v2))
                h = 0.5 + 0.5 * t
                slope = h * (1.0 + v * (1.0 - t) * (ROOT + (3.0 * ROOT * CUBIC) * v2))
                bg = co * m * slope
                bu = co * (v * h)
                new = tuple(
                    s + (back * moved).reshape(CHUNK // 8, 8, 128).sum(0)
                    for s, (back, moved) in zip(sums, [(bg, q) for q in sg] + [(bu, q) for q in su])
                )
                for ref, back, after, taps_of in ((pg, bg, next_g, kg), (pu, bu, next_u, ku)):
                    whole = jnp.concatenate([back, after], axis=0)
                    one = pltpu.roll(whole, CHUNK + 7, 0)[:CHUNK]
                    two = pltpu.roll(whole, CHUNK + 6, 0)[:CHUNK]
                    ref[here, cols] = (taps_of[2] * back + taps_of[1] * one + taps_of[0] * two).astype(bf16)
                return bg[:8], bu[:8], new

            zero = jnp.zeros((8, 128), f32)
            _, _, sums = lax.fori_loop(0, LEN // CHUNK, rows, (zero, zero, (zero,) * 6))
            rows8 = [jnp.sum(s, axis=0, keepdims=True) for s in sums]
            taps[0, x, :, cols] = jnp.concatenate(rows8 + [jnp.zeros((2, 128), f32)], axis=0)
            return 0

        lax.fori_loop(low, high, column, 0)

    grads = (pg, pu)

    def own_rows(p, s):
        parts = []
        for yb in range(4):
            chunk = wrap(first[p] - 1 - s) if yb < 2 else wrap(first[p] + 1 + s)
            parts.append(xt[pl.ds(mult(yb * 512 + chunk * 128, 128), 128), :])
        return jnp.concatenate(parts, axis=0)

    def product(p, k, s):
        at, width = SPLITS[k]
        right = grads[p][PAD : PAD + LEN, at : at + width]
        return jnp.dot(own_rows(p, s), right, preferred_element_type=f32).reshape(4, 128, width)

    def p1_send(k, p, s):
        for way in range(2):
            pair = pl.ds(way * 2, 2)
            send(
                bufs[k].at[p, s, pair], bufs[k].at[p, s + 1, pair], p1s.at[k * 2 + p], p1r.at[(k * 2 + p) * 3 + s],
                first_dev(p, 1 - 2 * way),
            )

    def step0(k):
        for p in range(2):
            bufs[k][p, 0] = product(p, k, 0).astype(bf16)
            p1_send(k, p, 0)

    def step1(k, s):
        at, width = SPLITS[k]
        for p in range(2):
            own[p, :, :, 0:width] = product(p, k, s)
        for p in range(2):
            received(bufs[k].at[p, s], p1r.at[(k * 2 + p) * 3 + s - 1])

            def add(yb, _):
                total = bufs[k][p, s, yb].astype(f32) + own[p, yb, :, 0:width]
                if s < 3:
                    bufs[k][p, s, yb] = total.astype(bf16)
                else:
                    acc1[p, yb, :, at : at + width] = total
                return 0

            lax.fori_loop(0, 4, add, 0)
            if s < 3:
                p1_send(k, p, s)

    def p2_send(k, p, s):
        for way in range(2):
            pair = pl.ds(way * 2, 2)
            send(
                twos[k].at[p, s, pair], twos[k].at[p, s + 1, pair], p2s.at[k * 2 + p], p2r.at[(k * 2 + p) * 3 + s],
                second_dev(p, 1 - 2 * way),
            )

    def step2(k, s):
        at, width = SPLITS[k]
        for p in range(2):
            if s > 0:
                received(twos[k].at[p, s], p2r.at[(k * 2 + p) * 3 + s - 1])

            def add(yb, _):
                move = (1 - 2 * (yb // 2)) * (1 + s)
                chunk = wrap(second[p] - move)
                total = acc1[p, yb, pl.ds(mult(chunk * 32, 32), 32), at : at + width]
                if s > 0:
                    total = total + twos[k][p, s, yb].astype(f32)
                if s < 3:
                    twos[k][p, s, yb] = total.astype(bf16)
                else:
                    acc2[p, yb, :, at : at + width] = total
                return 0

            lax.fori_loop(0, 4, add, 0)
            if s < 3:
                p2_send(k, p, s)

    def p3_send(k):
        at, width = SPLITS[k]
        for p in range(2):
            for d in (1, 3, 2):
                outs3[k][p, d - 1] = acc2[p, wrap(y + d), :, at : at + width].astype(bf16)
                send(
                    outs3[k].at[p, d - 1], ins3[k].at[p, d - 1], p3s.at[k * 2 + p], p3r.at[k * 2 + p], dev(dy=d)
                )

    def block(p, group, d_first, d_second, skip=0, rows=32):
        start = wrap(first[p] + d_first) * 128 + wrap(second[p] + d_second) * 32 + skip
        at, width = GROUPS[group]
        return ag.at[p, pl.ds(mult(start, 16), rows), pl.ds(at, width)]

    def amount(p, group, rows):
        at, width = GROUPS[group]
        return ag.at[p, pl.ds(0, rows), pl.ds(at, width)]

    def p3_finish(k, p):
        at, width = SPLITS[k]
        received(ins3[k].at[p], p3r.at[k * 2 + p])
        total = acc2[p, y, :, at : at + width]
        for d in (1, 3, 2):
            total = total + ins3[k][p, d - 1].astype(f32)
        start = mult(first[p] * 128 + second[p] * 32, 32)
        ag[p, pl.ds(start, 32), at : at + width] = total.astype(bf16)

    def a1_start(group, p):
        for d in (1, 3, 2):
            index = (group * 2 + p) * 3 + d - 1
            place = block(p, group, 0, 0)
            send(place, place, a1s.at[group * 2 + p], a1r.at[index], second_dev(p, d))

    def a1_wait(group, p, d):
        received(block(p, group, 0, -d), a1r.at[(group * 2 + p) * 3 + d - 1])

    def a2_start(group, p, d):
        place = block(p, group, 0, -d)
        for way in range(2):
            send(place, place, a2s.at[group * 2 + p], a2r.at[(group * 2 + p) * 4 + d], first_dev(p, 1 - 2 * way))

    def a2_pass_on(group, p, d):
        received(amount(p, group, 64), a2r.at[(group * 2 + p) * 4 + d])
        for way in range(2):
            from_ = 2 * way - 1
            part = block(p, group, from_, -d, 16 * way, 16)
            send(part, part, a3s.at[group * 2 + p], a3r.at[group * 2 + p], first_dev(p, -from_))

    def a3_wait(group, p):
        received(amount(p, group, 128), a3r.at[group * 2 + p])
        at, width = GROUPS[group]
        cols = pl.ds(at, width)
        pltpu.make_async_copy(ag.at[p, :, cols], ag_out.at[p, :, cols], osem.at[1]).start()

    coords = (x, z, y)

    def tap_dev(stage, d):
        return dev(dx=d) if stage == 0 else dev(dz=d) if stage == 1 else dev(dy=d)

    def tap_send(stage):
        place = taps.at[stage, coords[stage]]
        for d in (1, 2, 3):
            send(place, place, tss.at[stage], tsr.at[stage], tap_dev(stage, d))

    def tap_sum(stage):
        received(taps.at[stage, 0:3], tsr.at[stage])
        total = taps[stage, 0] + taps[stage, 1] + taps[stage, 2] + taps[stage, 3]
        if stage < 2:
            taps[stage + 1, coords[stage + 1]] = total
            tap_send(stage + 1)
        else:
            tfin[c] = total * (float(TOKENS) ** -0.5)
            send(tfin.at[c], tfin.at[c], tss.at[3], tsr.at[3], dev(dc=1))

    def tap_end():
        other = tfin.at[wrap(c + 1, 2)]
        received(other, tsr.at[3])
        pltpu.make_async_copy(tfin, tap_out, osem.at[2]).start()

    def project(unit, d, starts):
        shard = wrap(y + d)

        def weights(g):
            return jnp.concatenate([wall[g, shard, at : at + 128, :] for at in starts], axis=0)

        def side(which, _):
            to_partner = 1 - which
            row = mult(PAD + wrap(c + to_partner, 2) * HALF, 16)
            dims = (((1,), (1,)), ((), ()))
            value = lax.dot_general(pg[pl.ds(row, HALF), :], weights(0), dims, preferred_element_type=f32)
            value = value + lax.dot_general(pu[pl.ds(row, HALF), :], weights(1), dims, preferred_element_type=f32)
            gsend[which, unit] = value.astype(bf16)
            return 0

        lax.fori_loop(0, 2, side, 0)
        send(gsend.at[0, unit], grecv.at[unit], gss.at[0], gsr.at[unit], dev(dc=1))

    def combine(unit, d, starts):
        received(grecv.at[unit], gsr.at[unit])
        gown[unit] = (gsend[1, unit].astype(f32) + grecv[unit].astype(f32)).astype(bf16)
        for i, at in enumerate(starts):
            col = mult(wrap(y + d) * 512 + at, 128)
            part = gown.at[unit, :, pl.ds(i * 128, 128)]
            pltpu.make_async_copy(part, gi_out.at[:, pl.ds(col, 128)], osem.at[0]).start()

    def turn_half(side, count, block_of):
        rows = pl.ds(mult(side * HALF, HALF), HALF)

        def turn(i, _):
            at = pl.ds(mult(block_of(i) * 128, 128), 128)
            xt[at, rows] = xs[rows, at].T
            return 0

        lax.fori_loop(0, count, turn, 0)

    def early(i):
        yb = lax.rem(i, 4)
        base = jnp.where(i < 4, x, z)
        return yb * 4 + wrap(base - 1 + 2 * (yb // 2))

    def late(i):
        yb = i // 3
        return yb * 4 + wrap(x + lax.rem(i, 3) + 2 * (yb // 2))

    for copy in tap_loads + pre[0]:
        copy.wait()
    elementwise(0, 0, 2)
    x_local.wait()
    turn_half(c, 8, early)
    other_half = xs.at[pl.ds(mult(wrap(c + 1, 2) * HALF, HALF), HALF)]
    received(other_half, xsem.at[1])
    turn_half(wrap(c + 1, 2), 8, early)
    units = [(0, (0, 128)), (0, (256, 384)), (-1, (0, 128)), (1, (256, 384)), (-1, (256, 384)), (1, (0, 128))]
    units += [(2, (0, 256)), (2, (128, 384))]
    step0(0)
    for copy in pre[1]:
        copy.wait()
    elementwise(1, 0, 2)
    stripe_start()
    elementwise(1, 2, 4)
    step0(1)
    turn_half(0, 12, late)
    turn_half(1, 12, late)
    step1(0, 1)
    for copy in pre[2]:
        copy.wait()
    elementwise(2, 0, 2)
    stripe_pass()
    elementwise(2, 2, 5)
    step0(2)
    tap_send(0)
    step1(1, 1)
    step1(0, 2)
    for copy in w_local:
        copy.wait()
    step1(2, 1)
    project(0, *units[0])
    step1(1, 2)
    step1(0, 3)
    step2(0, 0)
    tap_sum(0)
    project(1, *units[1])
    step1(2, 2)
    for way in range(2):
        w_arrived(way, 0)
    w_forward(0)
    w_forward(1)
    project(2, *units[2])
    step1(1, 3)
    step2(1, 0)
    step2(0, 1)
    combine(0, *units[0])
    combine(1, *units[1])
    project(3, *units[3])
    step1(2, 3)
    step2(2, 0)
    step2(1, 1)
    step2(0, 2)
    tap_sum(1)
    step2(2, 1)
    step2(1, 2)
    step2(0, 3)
    p3_send(0)
    step2(2, 2)
    step2(1, 3)
    p3_send(1)
    step2(2, 3)
    p3_send(2)
    w_forward(2)
    stripe_end()
    for way in range(2):
        w_arrived(way, 1)
    project(4, *units[4])
    for p in range(2):
        for k in range(2):
            p3_finish(k, p)
        a1_start(0, p)
        a2_start(0, p, 0)
    combine(2, *units[2])
    combine(3, *units[3])
    for p in range(2):
        p3_finish(2, p)
        a1_start(1, p)
        a2_start(1, p, 0)
    for group in range(2):
        for d in (1, 3, 2):
            for p in range(2):
                a1_wait(group, p, d)
                a2_start(group, p, d)
    project(5, *units[5])
    tap_sum(2)
    for group in range(2):
        for d in (0, 1, 3, 2):
            for p in range(2):
                a2_pass_on(group, p, d)
    w_far_arrived(0)
    project(6, *units[6])
    combine(4, *units[4])
    combine(5, *units[5])
    tap_end()
    for p in range(2):
        a3_wait(0, p)
    w_far_arrived(1)
    w_far_arrived(2)
    project(7, *units[7])
    for p in range(2):
        a3_wait(1, p)
    combine(6, *units[6])
    sent(xs.at[mine], xsem.at[0])
    sent(wall.at[:, 0:2, 0 : 512 - 3 * STRIPE], ws.at[0])
    sent(wall.at[:, 0, 0 : 4 * STRIPE], ws.at[1])
    sent(wall.at[0, 0, 0 : 4 * STRIPE], ws.at[2])
    sent(wall.at[:, 0], ws.at[3])
    for k in range(len(SPLITS)):
        for p in range(2):
            sent(bufs[k].at[p, 0:3], p1s.at[k * 2 + p])
            sent(twos[k].at[p, 0:3], p2s.at[k * 2 + p])
            sent(outs3[k].at[p], p3s.at[k * 2 + p])
    for group in range(2):
        for p in range(2):
            sent(amount(p, group, 96), a1s.at[group * 2 + p])
            sent(amount(p, group, 256), a2s.at[group * 2 + p])
            sent(amount(p, group, 128), a3s.at[group * 2 + p])
    for stage in range(3):
        sent(taps.at[stage, 0:3], tss.at[stage])
    sent(tfin.at[0], tss.at[3])
    sent(gsend.at[0], gss.at[0])
    combine(7, *units[7])
    for sem, ref in enumerate((gown, ag, tfin)):
        pltpu.make_async_copy(ref, ref, osem.at[sem]).wait()


def finish(gi_in, ag_in, tap_in, gi_out, gate_out, up_out, tap_gate, tap_up, gi, half, full, tap, tg, tu, sems):
    copies, count = [], 8
    rows = 512 // count

    def start(src, dst):
        copy = pltpu.make_async_copy(src, dst, sems.at[len(copies)])
        copy.start()
        copies.append(copy)
        return copy

    tap_load = start(tap_in, tap)
    loads = []
    for i in range(count):
        part = pl.ds(i * rows, rows)
        loads.append(start(ag_in.at[:, part], half.at[:, part]))
    gi_load = start(gi_in, gi)
    tap_load.wait()
    for side in range(2):
        cols = slice(side * COLS, side * COLS + COLS)
        tg[:, cols] = tap[side, 0:3]
        tu[:, cols] = tap[side, 3:6]
    stores = [start(tg, tap_gate), start(tu, tap_up)]
    for i in range(count):
        part = pl.ds(i * rows, rows)
        loads[i].wait()
        for p, target in enumerate((gate_out, up_out)):
            full[p, part] = half[p, part].astype(f32) * (float(TOKENS) ** -0.5)
            stores.append(start(full.at[p, part], target.at[part]))
    gi_load.wait()
    stores.append(start(gi, gi_out.at[0]))
    for copy in stores:
        copy.wait()


def per_device(inputs, pre_gate, pre_up, cotangent, w_gate, w_up, taps_gate, taps_up):
    any_ = pl.BlockSpec(memory_space=pl.ANY)
    dma = pltpu.SemaphoreType.DMA
    widths = [width for _, width in SPLITS]
    count = len(widths)
    scratch = (
        [pltpu.VMEM((PAD + LEN, COLS), bf16)] * 3
        + [pltpu.VMEM((LEN, WIDTH), bf16), pltpu.VMEM((WIDTH, LEN), bf16), pltpu.VMEM((2, 4, 512, COLS), bf16)]
        + [pltpu.VMEM((2, 4, 4, 128, width), bf16) for width in widths]
        + [pltpu.VMEM((2, 4, 128, max(widths)), f32), pltpu.VMEM((2, 4, 128, COLS), f32)]
        + [pltpu.VMEM((2, 4, 4, 32, width), bf16) for width in widths]
        + [pltpu.VMEM((2, 4, 32, COLS), f32)]
        + [pltpu.VMEM((2, 3, 32, width), bf16) for width in widths] * 2
        + [pltpu.VMEM((2, 512, COLS), bf16), pltpu.VMEM((3, 4, 8, COLS), f32), pltpu.VMEM((2, 8, COLS), f32)]
        + [pltpu.VMEM((2, 8, HALF, 256), bf16), pltpu.VMEM((8, HALF, 256), bf16), pltpu.VMEM((8, HALF, 256), bf16)]
        + [pltpu.VMEM((3, 2 * COLS), bf16)] * 2
        + [dma((14,)), dma((3,)), dma((2,)), dma((4,)), dma((2,)), dma((4,)), dma((2 * len(FAR),)), dma((4,)), dma((4,))]
        + [dma((2 * count,)), dma((6 * count,))] * 2
        + [dma((2 * count,)), dma((2 * count,))]
        + [dma((4,)), dma((12,)), dma((4,)), dma((16,)), dma((4,)), dma((4,)), dma((4,)), dma((4,)), dma((1,)), dma((8,))]
    )
    grad_inputs, sums, tap_sums = pl.pallas_call(
        kernel,
        out_shape=(
            jax.ShapeDtypeStruct((HALF, WIDTH), bf16),
            jax.ShapeDtypeStruct((2, 512, COLS), bf16),
            jax.ShapeDtypeStruct((2, 8, COLS), f32),
        ),
        in_specs=[any_] * 8,
        out_specs=(any_,) * 3,
        scratch_shapes=scratch,
        compiler_params=pltpu.CompilerParams(
            collective_id=0, has_side_effects=True, vmem_limit_bytes=67043328
        ),
    )(inputs, pre_gate, pre_up, cotangent, w_gate, w_up, taps_gate, taps_up)
    return tuple(
        pl.pallas_call(
            finish,
            out_shape=(
                jax.ShapeDtypeStruct((1, HALF, WIDTH), bf16),
                jax.ShapeDtypeStruct((512, COLS), f32),
                jax.ShapeDtypeStruct((512, COLS), f32),
                jax.ShapeDtypeStruct((3, 2 * COLS), f32),
                jax.ShapeDtypeStruct((3, 2 * COLS), f32),
            ),
            in_specs=[any_] * 3,
            out_specs=(any_,) * 5,
            scratch_shapes=[
                pltpu.VMEM((HALF, WIDTH), bf16),
                pltpu.VMEM((2, 512, COLS), bf16),
                pltpu.VMEM((2, 512, COLS), f32),
                pltpu.VMEM((2, 8, COLS), f32),
                pltpu.VMEM((3, 2 * COLS), f32),
                pltpu.VMEM((3, 2 * COLS), f32),
                dma((32,)),
            ],
            compiler_params=pltpu.CompilerParams(vmem_limit_bytes=67043328),
        )(grad_inputs, sums, tap_sums)
    )


def solution(mesh):
    placed = (
        P(("rep", "fs"), "tp", None),
        P(("rep", "fs"), None, "tp"),
        P(("rep", "fs"), None, "tp"),
        P(("rep", "fs"), None, "tp"),
        P("fs", "tp"),
        P("fs", "tp"),
        P(),
        P(),
    )
    return jax.shard_map(
        per_device,
        mesh=mesh,
        in_specs=placed,
        out_specs=(P(("rep", "fs"), "tp", None), P("fs", "tp"), P("fs", "tp"), P(), P()),
        check_vma=False,
    )
```

```python
import functools

import jax
import jax.numpy as jnp
from jax import lax
from jax.experimental import pallas as pl
from jax.experimental.pallas import tpu as pltpu
from jax.sharding import PartitionSpec as P

MESH = pl.DeviceIdType.MESH
LEN = 768
COLS = 1408
WIDTH = 2048
TOKENS = 49152
SPLITS = ((0, 256), (256, 512), (768, 640))
CHUNK = 64
PAD = 16
STRIPE = 32
FAR = ((0, 128), (128, 32), (160, 32), (192, 64))
GROUPS = ((0, 768), (768, 640))
HALF = LEN // 2
ROOT = 0.7978845608028654
CUBIC = 0.044715
bf16, f32 = jnp.bfloat16, jnp.float32


def wrap(value, n=4):
    return lax.rem(value + 2 * n, n)


def mult(value, n):
    return pl.multiple_of(value, n)


def kernel(
    x_hbm, pg_hbm, pu_hbm, ct_hbm, wg_hbm, wu_hbm, tg_hbm, tu_hbm,
    gi_out, ag_out, tap_out,
    pg, pu, ct, xs, xt, wall, buf0, buf1, buf2, own, acc1, two0, two1, two2, acc2,
    out3_0, out3_1, out3_2, in3_0, in3_1, in3_2, ag, taps, tfin, gsend, gown, grecv, tg_ref, tu_ref,
    loc, osem, xsem, ws, w0r, w1r, w2r, w3r, w4r, p1s, p1r, p2s, p2r, p3s, p3r,
    a1s, a1r, a2s, a2r, a3s, a3r, tss, tsr, gss, gsr,
):
    rep, y, c = lax.axis_index("rep"), lax.axis_index("fs"), lax.axis_index("tp")
    z, x = rep // 4, lax.rem(rep, 4)
    first, second = (x, z), (z, x)
    bufs, twos = (buf0, buf1, buf2), (two0, two1, two2)
    outs3, ins3 = (out3_0, out3_1, out3_2), (in3_0, in3_1, in3_2)

    def dev(dx=0, dz=0, dy=0, dc=0):
        return (wrap(z + dz) * 4 + wrap(x + dx), wrap(y + dy), wrap(c + dc, 2))

    def first_dev(p, d):
        return dev(dx=d) if p == 0 else dev(dz=d)

    def second_dev(p, d):
        return dev(dz=d) if p == 0 else dev(dx=d)

    def remote(src, dst, send, recv, where):
        return pltpu.make_async_remote_copy(
            src_ref=src, dst_ref=dst, send_sem=send, recv_sem=recv, device_id=where, device_id_type=MESH
        )

    def send(src, dst, send_sem, recv_sem, where):
        remote(src, dst, send_sem, recv_sem, where).start()

    def received(place, sem):
        remote(place, place, sem, sem, dev(dc=1)).wait_recv()

    def sent(place, sem):
        remote(place, place, sem, sem, dev(dc=1)).wait_send()

    local = []

    def load(src, dst):
        copy = pltpu.make_async_copy(src, dst, loc.at[len(local)])
        copy.start()
        local.append(copy)
        return copy

    tap_loads = [load(tg_hbm, tg_ref), load(tu_hbm, tu_ref)]
    pre = []
    for at, width in SPLITS:
        cols = pl.ds(at, width)
        pre.append(
            [load(h.at[0, :, cols], v.at[pl.ds(PAD, LEN), cols]) for h, v in ((pg_hbm, pg), (pu_hbm, pu), (ct_hbm, ct))]
        )
    mine = pl.ds(mult(c * HALF, HALF), HALF)
    x_local = load(x_hbm.at[0], xs.at[mine])
    w_local = [load(h, wall.at[g, y]) for g, h in enumerate((wg_hbm, wu_hbm))]
    pg[0:PAD, :] = jnp.zeros((PAD, COLS), bf16)
    pu[0:PAD, :] = jnp.zeros((PAD, COLS), bf16)

    peers = [dev(dx=d) for d in (1, 2, 3)] + [dev(dz=d) for d in (1, 2, 3)]
    peers += [dev(dy=d) for d in (1, 2, 3)] + [dev(dc=1)]
    barrier = pltpu.get_barrier_semaphore()
    for peer in peers:
        pl.semaphore_signal(barrier, inc=1, device_id=peer, device_id_type=MESH)
    pl.semaphore_wait(barrier, len(peers))

    send(x_hbm.at[0], xs.at[mine], xsem.at[0], xsem.at[1], dev(dc=1))
    ways = ((-1, x, 0, 512 - 4 * STRIPE), (1, z, 256, 0))

    def ring_dev(way, d):
        return dev(dx=d) if way == 0 else dev(dz=d)

    def stripe(way, d):
        source, at, _, base = ways[way]
        return wrap(y + source), pl.ds(mult(base + wrap(at + d) * STRIPE, STRIPE), STRIPE)

    def passed(way):
        source, _, start, _ = ways[way]
        return wrap(y + source), pl.ds(start, 256)

    def rest(way):
        source = ways[way][0]
        return wrap(y + source), pl.ds(256 if way == 0 else 4 * STRIPE, 256 - 4 * STRIPE)

    for level, rows_of in enumerate((lambda way: stripe(way, 0), passed, rest)):
        for g, h in enumerate((wg_hbm, wu_hbm)):
            for way in range(2):
                rows = rows_of(way)[1]
                sem = w0r.at[way] if level == 0 else w1r.at[way * 2 + level - 1]
                send(h.at[rows], wall.at[g, y, rows], ws.at[0], sem, dev(dy=-ways[way][0]))

    def stripe_start():
        for way in range(2):
            shard, rows = stripe(way, 0)
            place = wall.at[:, shard, rows]
            received(place, w0r.at[way])
            for side, d in enumerate((1, -1)):
                send(place, place, ws.at[1], w3r.at[way * 2 + side], ring_dev(way, d))

    def stripe_pass():
        for way in range(2):
            for side, d in enumerate((1, -1)):
                shard, rows = stripe(way, -d)
                received(wall.at[:, shard, rows], w3r.at[way * 2 + side])
                place = wall.at[side, shard, rows]
                send(place, place, ws.at[2], w4r.at[way * 2 + side], ring_dev(way, d))

    def stripe_end():
        for way in range(2):
            shard, rows = stripe(way, 2)
            for side in range(2):
                received(wall.at[side, shard, rows], w4r.at[way * 2 + side])

    def w_arrived(way, level):
        shard, rows = (passed, rest)[level](way)
        received(wall.at[:, shard, rows], w1r.at[way * 2 + level])

    def w_forward(piece):
        at, count = FAR[piece]
        for way in range(2):
            place = wall.at[:, wrap(y + ways[way][0]), pl.ds(way * 256 + at, count)]
            send(place, place, ws.at[3], w2r.at[way * len(FAR) + piece], dev(dy=-ways[way][0]))

    def w_far_arrived(piece):
        at, count = FAR[piece]
        for way in range(2):
            received(wall.at[:, wrap(y + 2), pl.ds(way * 256 + at, count)], w2r.at[way * len(FAR) + piece])

    def elementwise(k, low, high):
        at = SPLITS[k][0]

        def column(b, _):
            col = mult(at + b * 128, 128)
            cols = pl.ds(col, 128)
            shared = pl.ds(mult(c * COLS + col, 128), 128)
            kg = tg_ref[:, shared].astype(f32)
            ku = tu_ref[:, shared].astype(f32)
            kg = [kg[j : j + 1] for j in range(3)]
            ku = [ku[j : j + 1] for j in range(3)]

            def rows(i, carry):
                next_g, next_u, sums = carry
                r = mult(LEN - CHUNK - i * CHUNK, CHUNK)
                span, here = pl.ds(r, CHUNK + PAD), pl.ds(r + PAD, CHUNK)
                eg = pg[span, cols].astype(f32)[8:]
                eu = pu[span, cols].astype(f32)[8:]
                co = ct[here, cols].astype(f32)
                sg = [pltpu.roll(eg, 2, 0)[8:], pltpu.roll(eg, 1, 0)[8:], eg[8:]]
                su = [pltpu.roll(eu, 2, 0)[8:], pltpu.roll(eu, 1, 0)[8:], eu[8:]]
                v = kg[0] * sg[0] + kg[1] * sg[1] + kg[2] * sg[2]
                m = ku[0] * su[0] + ku[1] * su[1] + ku[2] * su[2]
                v2 = v * v
                t = jnp.tanh(v * (ROOT + (ROOT * CUBIC) * v2))
                h = 0.5 + 0.5 * t
                slope = h * (1.0 + v * (1.0 - t) * (ROOT + (3.0 * ROOT * CUBIC) * v2))
                bg = co * m * slope
                bu = co * (v * h)
                new = tuple(
                    s + (back * moved).reshape(CHUNK // 8, 8, 128).sum(0)
                    for s, (back, moved) in zip(sums, [(bg, q) for q in sg] + [(bu, q) for q in su])
                )
                for ref, back, after, taps_of in ((pg, bg, next_g, kg), (pu, bu, next_u, ku)):
                    whole = jnp.concatenate([back, after], axis=0)
                    one = pltpu.roll(whole, CHUNK + 7, 0)[:CHUNK]
                    two = pltpu.roll(whole, CHUNK + 6, 0)[:CHUNK]
                    ref[here, cols] = (taps_of[2] * back + taps_of[1] * one + taps_of[0] * two).astype(bf16)
                return bg[:8], bu[:8], new

            zero = jnp.zeros((8, 128), f32)
            _, _, sums = lax.fori_loop(0, LEN // CHUNK, rows, (zero, zero, (zero,) * 6))
            rows8 = [jnp.sum(s, axis=0, keepdims=True) for s in sums]
            taps[0, x, :, cols] = jnp.concatenate(rows8 + [jnp.zeros((2, 128), f32)], axis=0)
            return 0

        lax.fori_loop(low, high, column, 0)

    grads = (pg, pu)

    def own_rows(p, s):
        parts = []
        for yb in range(4):
            chunk = wrap(first[p] - 1 - s) if yb < 2 else wrap(first[p] + 1 + s)
            parts.append(xt[pl.ds(mult(yb * 512 + chunk * 128, 128), 128), :])
        return jnp.concatenate(parts, axis=0)

    def product(p, k, s):
        at, width = SPLITS[k]
        right = grads[p][PAD : PAD + LEN, at : at + width]
        return jnp.dot(own_rows(p, s), right, preferred_element_type=f32).reshape(4, 128, width)

    def p1_send(k, p, s):
        for way in range(2):
            pair = pl.ds(way * 2, 2)
            send(
                bufs[k].at[p, s, pair], bufs[k].at[p, s + 1, pair], p1s.at[k * 2 + p], p1r.at[(k * 2 + p) * 3 + s],
                first_dev(p, 1 - 2 * way),
            )

    def step0(k):
        for p in range(2):
            bufs[k][p, 0] = product(p, k, 0).astype(bf16)
            p1_send(k, p, 0)

    def step1(k, s):
        at, width = SPLITS[k]
        for p in range(2):
            own[p, :, :, 0:width] = product(p, k, s)
        for p in range(2):
            received(bufs[k].at[p, s], p1r.at[(k * 2 + p) * 3 + s - 1])

            def add(yb, _):
                total = bufs[k][p, s, yb].astype(f32) + own[p, yb, :, 0:width]
                if s < 3:
                    bufs[k][p, s, yb] = total.astype(bf16)
                else:
                    acc1[p, yb, :, at : at + width] = total
                return 0

            lax.fori_loop(0, 4, add, 0)
            if s < 3:
                p1_send(k, p, s)

    def p2_send(k, p, s):
        for way in range(2):
            pair = pl.ds(way * 2, 2)
            send(
                twos[k].at[p, s, pair], twos[k].at[p, s + 1, pair], p2s.at[k * 2 + p], p2r.at[(k * 2 + p) * 3 + s],
                second_dev(p, 1 - 2 * way),
            )

    def step2(k, s):
        at, width = SPLITS[k]
        for p in range(2):
            if s > 0:
                received(twos[k].at[p, s], p2r.at[(k * 2 + p) * 3 + s - 1])

            def add(yb, _):
                move = (1 - 2 * (yb // 2)) * (1 + s)
                chunk = wrap(second[p] - move)
                total = acc1[p, yb, pl.ds(mult(chunk * 32, 32), 32), at : at + width]
                if s > 0:
                    total = total + twos[k][p, s, yb].astype(f32)
                if s < 3:
                    twos[k][p, s, yb] = total.astype(bf16)
                else:
                    acc2[p, yb, :, at : at + width] = total
                return 0

            lax.fori_loop(0, 4, add, 0)
            if s < 3:
                p2_send(k, p, s)

    def p3_send(k):
        at, width = SPLITS[k]
        for p in range(2):
            for d in (1, 3, 2):
                outs3[k][p, d - 1] = acc2[p, wrap(y + d), :, at : at + width].astype(bf16)
                send(
                    outs3[k].at[p, d - 1], ins3[k].at[p, d - 1], p3s.at[k * 2 + p], p3r.at[k * 2 + p], dev(dy=d)
                )

    def block(p, group, d_first, d_second, skip=0, rows=32):
        start = wrap(first[p] + d_first) * 128 + wrap(second[p] + d_second) * 32 + skip
        at, width = GROUPS[group]
        return ag.at[p, pl.ds(mult(start, 16), rows), pl.ds(at, width)]

    def amount(p, group, rows):
        at, width = GROUPS[group]
        return ag.at[p, pl.ds(0, rows), pl.ds(at, width)]

    def p3_finish(k, p):
        at, width = SPLITS[k]
        received(ins3[k].at[p], p3r.at[k * 2 + p])
        total = acc2[p, y, :, at : at + width]
        for d in (1, 3, 2):
            total = total + ins3[k][p, d - 1].astype(f32)
        start = mult(first[p] * 128 + second[p] * 32, 32)
        ag[p, pl.ds(start, 32), at : at + width] = total.astype(bf16)

    def a1_start(group, p):
        for d in (1, 3, 2):
            index = (group * 2 + p) * 3 + d - 1
            place = block(p, group, 0, 0)
            send(place, place, a1s.at[group * 2 + p], a1r.at[index], second_dev(p, d))

    def a1_wait(group, p, d):
        received(block(p, group, 0, -d), a1r.at[(group * 2 + p) * 3 + d - 1])

    def a2_start(group, p, d):
        place = block(p, group, 0, -d)
        for way in range(2):
            send(place, place, a2s.at[group * 2 + p], a2r.at[(group * 2 + p) * 4 + d], first_dev(p, 1 - 2 * way))

    def a2_pass_on(group, p, d):
        received(amount(p, group, 64), a2r.at[(group * 2 + p) * 4 + d])
        for way in range(2):
            from_ = 2 * way - 1
            part = block(p, group, from_, -d, 16 * way, 16)
            send(part, part, a3s.at[group * 2 + p], a3r.at[group * 2 + p], first_dev(p, -from_))

    def a3_wait(group, p):
        received(amount(p, group, 128), a3r.at[group * 2 + p])
        at, width = GROUPS[group]
        cols = pl.ds(at, width)
        pltpu.make_async_copy(ag.at[p, :, cols], ag_out.at[p, :, cols], osem.at[1]).start()

    coords = (x, z, y)

    def tap_dev(stage, d):
        return dev(dx=d) if stage == 0 else dev(dz=d) if stage == 1 else dev(dy=d)

    def tap_send(stage):
        place = taps.at[stage, coords[stage]]
        for d in (1, 2, 3):
            send(place, place, tss.at[stage], tsr.at[stage], tap_dev(stage, d))

    def tap_sum(stage):
        received(taps.at[stage, 0:3], tsr.at[stage])
        total = taps[stage, 0] + taps[stage, 1] + taps[stage, 2] + taps[stage, 3]
        if stage < 2:
            taps[stage + 1, coords[stage + 1]] = total
            tap_send(stage + 1)
        else:
            tfin[c] = total * (float(TOKENS) ** -0.5)
            send(tfin.at[c], tfin.at[c], tss.at[3], tsr.at[3], dev(dc=1))

    def tap_end():
        other = tfin.at[wrap(c + 1, 2)]
        received(other, tsr.at[3])
        pltpu.make_async_copy(tfin, tap_out, osem.at[2]).start()

    def project(unit, d, starts):
        shard = wrap(y + d)

        def weights(g):
            return jnp.concatenate([wall[g, shard, at : at + 128, :] for at in starts], axis=0)

        def side(which, _):
            to_partner = 1 - which
            row = mult(PAD + wrap(c + to_partner, 2) * HALF, 16)
            dims = (((1,), (1,)), ((), ()))
            value = lax.dot_general(pg[pl.ds(row, HALF), :], weights(0), dims, preferred_element_type=f32)
            value = value + lax.dot_general(pu[pl.ds(row, HALF), :], weights(1), dims, preferred_element_type=f32)
            gsend[which, unit] = value.astype(bf16)
            return 0

        lax.fori_loop(0, 2, side, 0)
        send(gsend.at[0, unit], grecv.at[unit], gss.at[0], gsr.at[unit], dev(dc=1))

    def combine(unit, d, starts):
        received(grecv.at[unit], gsr.at[unit])
        gown[unit] = (gsend[1, unit].astype(f32) + grecv[unit].astype(f32)).astype(bf16)
        for i, at in enumerate(starts):
            col = mult(wrap(y + d) * 512 + at, 128)
            part = gown.at[unit, :, pl.ds(i * 128, 128)]
            pltpu.make_async_copy(part, gi_out.at[:, pl.ds(col, 128)], osem.at[0]).start()

    def turn_half(side, count, block_of):
        rows = pl.ds(mult(side * HALF, HALF), HALF)

        def turn(i, _):
            at = pl.ds(mult(block_of(i) * 128, 128), 128)
            xt[at, rows] = xs[rows, at].T
            return 0

        lax.fori_loop(0, count, turn, 0)

    def early(i):
        yb = lax.rem(i, 4)
        base = jnp.where(i < 4, x, z)
        return yb * 4 + wrap(base - 1 + 2 * (yb // 2))

    def late(i):
        yb = i // 3
        return yb * 4 + wrap(x + lax.rem(i, 3) + 2 * (yb // 2))

    for copy in tap_loads + pre[0]:
        copy.wait()
    elementwise(0, 0, 2)
    x_local.wait()
    turn_half(c, 8, early)
    other_half = xs.at[pl.ds(mult(wrap(c + 1, 2) * HALF, HALF), HALF)]
    received(other_half, xsem.at[1])
    turn_half(wrap(c + 1, 2), 8, early)
    units = [(0, (0, 128)), (0, (256, 384)), (-1, (0, 128)), (1, (256, 384)), (-1, (256, 384)), (1, (0, 128))]
    units += [(2, (0, 256)), (2, (128, 384))]
    step0(0)
    for copy in pre[1]:
        copy.wait()
    elementwise(1, 0, 2)
    stripe_start()
    elementwise(1, 2, 4)
    step0(1)
    turn_half(0, 12, late)
    turn_half(1, 12, late)
    step1(0, 1)
    for copy in pre[2]:
        copy.wait()
    elementwise(2, 0, 2)
    stripe_pass()
    elementwise(2, 2, 5)
    step0(2)
    step1(1, 1)
    step1(0, 2)
    for copy in w_local:
        copy.wait()
    project(0, *units[0])
    project(1, *units[1])
    step1(2, 1)
    step1(1, 2)
    for way in range(2):
        w_arrived(way, 0)
    w_forward(0)
    project(2, *units[2])
    step1(0, 3)
    step2(0, 0)
    project(3, *units[3])
    step1(2, 2)
    combine(0, *units[0])
    combine(1, *units[1])
    step1(1, 3)
    step2(1, 0)
    step2(0, 1)
    stripe_end()
    for way in range(2):
        w_arrived(way, 1)
    project(4, *units[4])
    combine(2, *units[2])
    combine(3, *units[3])
    step1(2, 3)
    step2(2, 0)
    w_forward(1)
    step2(1, 1)
    step2(0, 2)
    step2(2, 1)
    step2(1, 2)
    step2(0, 3)
    p3_send(0)
    step2(2, 2)
    step2(1, 3)
    p3_send(1)
    step2(2, 3)
    p3_send(2)
    tap_send(0)
    w_forward(2)
    w_forward(3)
    project(5, *units[5])
    for p in range(2):
        for k in range(2):
            p3_finish(k, p)
        a1_start(0, p)
        a2_start(0, p, 0)
    for p in range(2):
        p3_finish(2, p)
        a1_start(1, p)
        a2_start(1, p, 0)
    tap_sum(0)
    w_far_arrived(0)
    for d in (1, 3, 2):
        for p in range(2):
            a1_wait(0, p, d)
            a2_start(0, p, d)
    project(6, *units[6])
    for d in (1, 3, 2):
        for p in range(2):
            a1_wait(1, p, d)
            a2_start(1, p, d)
    tap_sum(1)
    combine(4, *units[4])
    combine(5, *units[5])
    for d in (0, 1, 3, 2):
        for p in range(2):
            a2_pass_on(0, p, d)
    tap_sum(2)
    for d in (0, 1, 3, 2):
        for p in range(2):
            a2_pass_on(1, p, d)
    for piece in range(1, len(FAR)):
        w_far_arrived(piece)
    project(7, *units[7])
    combine(6, *units[6])
    tap_end()
    for group in range(2):
        for p in range(2):
            a3_wait(group, p)
    sent(xs.at[mine], xsem.at[0])
    sent(wall.at[:, 0:2, 0 : 512 - 3 * STRIPE], ws.at[0])
    sent(wall.at[:, 0, 0 : 4 * STRIPE], ws.at[1])
    sent(wall.at[0, 0, 0 : 4 * STRIPE], ws.at[2])
    sent(wall.at[:, 0], ws.at[3])
    for k in range(len(SPLITS)):
        for p in range(2):
            sent(bufs[k].at[p, 0:3], p1s.at[k * 2 + p])
            sent(twos[k].at[p, 0:3], p2s.at[k * 2 + p])
            sent(outs3[k].at[p], p3s.at[k * 2 + p])
    for group in range(2):
        for p in range(2):
            sent(amount(p, group, 96), a1s.at[group * 2 + p])
            sent(amount(p, group, 256), a2s.at[group * 2 + p])
            sent(amount(p, group, 128), a3s.at[group * 2 + p])
    for stage in range(3):
        sent(taps.at[stage, 0:3], tss.at[stage])
    sent(tfin.at[0], tss.at[3])
    sent(gsend.at[0], gss.at[0])
    combine(7, *units[7])
    for sem, ref in enumerate((gown, ag, tfin)):
        pltpu.make_async_copy(ref, ref, osem.at[sem]).wait()


def finish(gi_in, ag_in, tap_in, gi_out, gate_out, up_out, tap_gate, tap_up, gi, half, full, tap, tg, tu, sems):
    copies, count = [], 8
    rows = 512 // count

    def start(src, dst):
        copy = pltpu.make_async_copy(src, dst, sems.at[len(copies)])
        copy.start()
        copies.append(copy)
        return copy

    tap_load = start(tap_in, tap)
    loads = []
    for i in range(count):
        part = pl.ds(i * rows, rows)
        loads.append(start(ag_in.at[:, part], half.at[:, part]))
    gi_load = start(gi_in, gi)
    tap_load.wait()
    for side in range(2):
        cols = slice(side * COLS, side * COLS + COLS)
        tg[:, cols] = tap[side, 0:3]
        tu[:, cols] = tap[side, 3:6]
    stores = [start(tg, tap_gate), start(tu, tap_up)]
    for i in range(count):
        part = pl.ds(i * rows, rows)
        loads[i].wait()
        for p, target in enumerate((gate_out, up_out)):
            full[p, part] = half[p, part].astype(f32) * (float(TOKENS) ** -0.5)
            stores.append(start(full.at[p, part], target.at[part]))
    gi_load.wait()
    stores.append(start(gi, gi_out.at[0]))
    for copy in stores:
        copy.wait()


def per_device(inputs, pre_gate, pre_up, cotangent, w_gate, w_up, taps_gate, taps_up):
    any_ = pl.BlockSpec(memory_space=pl.ANY)
    dma = pltpu.SemaphoreType.DMA
    widths = [width for _, width in SPLITS]
    count = len(widths)
    scratch = (
        [pltpu.VMEM((PAD + LEN, COLS), bf16)] * 3
        + [pltpu.VMEM((LEN, WIDTH), bf16), pltpu.VMEM((WIDTH, LEN), bf16), pltpu.VMEM((2, 4, 512, COLS), bf16)]
        + [pltpu.VMEM((2, 4, 4, 128, width), bf16) for width in widths]
        + [pltpu.VMEM((2, 4, 128, max(widths)), f32), pltpu.VMEM((2, 4, 128, COLS), f32)]
        + [pltpu.VMEM((2, 4, 4, 32, width), bf16) for width in widths]
        + [pltpu.VMEM((2, 4, 32, COLS), f32)]
        + [pltpu.VMEM((2, 3, 32, width), bf16) for width in widths] * 2
        + [pltpu.VMEM((2, 512, COLS), bf16), pltpu.VMEM((3, 4, 8, COLS), f32), pltpu.VMEM((2, 8, COLS), f32)]
        + [pltpu.VMEM((2, 8, HALF, 256), bf16), pltpu.VMEM((8, HALF, 256), bf16), pltpu.VMEM((8, HALF, 256), bf16)]
        + [pltpu.VMEM((3, 2 * COLS), bf16)] * 2
        + [dma((14,)), dma((3,)), dma((2,)), dma((4,)), dma((2,)), dma((4,)), dma((2 * len(FAR),)), dma((4,)), dma((4,))]
        + [dma((2 * count,)), dma((6 * count,))] * 2
        + [dma((2 * count,)), dma((2 * count,))]
        + [dma((4,)), dma((12,)), dma((4,)), dma((16,)), dma((4,)), dma((4,)), dma((4,)), dma((4,)), dma((1,)), dma((8,))]
    )
    grad_inputs, sums, tap_sums = pl.pallas_call(
        kernel,
        out_shape=(
            jax.ShapeDtypeStruct((HALF, WIDTH), bf16),
            jax.ShapeDtypeStruct((2, 512, COLS), bf16),
            jax.ShapeDtypeStruct((2, 8, COLS), f32),
        ),
        in_specs=[any_] * 8,
        out_specs=(any_,) * 3,
        scratch_shapes=scratch,
        compiler_params=pltpu.CompilerParams(
            collective_id=0, has_side_effects=True, vmem_limit_bytes=67043328
        ),
    )(inputs, pre_gate, pre_up, cotangent, w_gate, w_up, taps_gate, taps_up)
    return tuple(
        pl.pallas_call(
            finish,
            out_shape=(
                jax.ShapeDtypeStruct((1, HALF, WIDTH), bf16),
                jax.ShapeDtypeStruct((512, COLS), f32),
                jax.ShapeDtypeStruct((512, COLS), f32),
                jax.ShapeDtypeStruct((3, 2 * COLS), f32),
                jax.ShapeDtypeStruct((3, 2 * COLS), f32),
            ),
            in_specs=[any_] * 3,
            out_specs=(any_,) * 5,
            scratch_shapes=[
                pltpu.VMEM((HALF, WIDTH), bf16),
                pltpu.VMEM((2, 512, COLS), bf16),
                pltpu.VMEM((2, 512, COLS), f32),
                pltpu.VMEM((2, 8, COLS), f32),
                pltpu.VMEM((3, 2 * COLS), f32),
                pltpu.VMEM((3, 2 * COLS), f32),
                dma((32,)),
            ],
            compiler_params=pltpu.CompilerParams(vmem_limit_bytes=67043328),
        )(grad_inputs, sums, tap_sums)
    )


def solution(mesh):
    placed = (
        P(("rep", "fs"), "tp", None),
        P(("rep", "fs"), None, "tp"),
        P(("rep", "fs"), None, "tp"),
        P(("rep", "fs"), None, "tp"),
        P("fs", "tp"),
        P("fs", "tp"),
        P(),
        P(),
    )
    return jax.shard_map(
        per_device,
        mesh=mesh,
        in_specs=placed,
        out_specs=(P(("rep", "fs"), "tp", None), P("fs", "tp"), P("fs", "tp"), P(), P()),
        check_vma=False,
    )
```

```python
import functools

import jax
import jax.numpy as jnp
from jax import lax
from jax.experimental import pallas as pl
from jax.experimental.pallas import tpu as pltpu
from jax.sharding import PartitionSpec as P

MESH = pl.DeviceIdType.MESH
LEN = 768
COLS = 1408
WIDTH = 2048
TOKENS = 49152
SPLITS = ((0, 256), (256, 512), (768, 640))
CHUNK = 64
PAD = 16
STRIPE = 32
FAR = ((0, 128), (128, 32), (160, 32), (192, 64))
GROUPS = SPLITS
HALF = LEN // 2
ROOT = 0.7978845608028654
CUBIC = 0.044715
bf16, f32 = jnp.bfloat16, jnp.float32


def wrap(value, n=4):
    return lax.rem(value + 2 * n, n)


def mult(value, n):
    return pl.multiple_of(value, n)


def kernel(
    x_hbm, pg_hbm, pu_hbm, ct_hbm, wg_hbm, wu_hbm, tg_hbm, tu_hbm,
    gi_out, ag_out, tap_out,
    pg, pu, ct, xs, xt, wall, buf0, buf1, buf2, own, acc1, two0, two1, two2, acc2,
    out3_0, out3_1, out3_2, in3_0, in3_1, in3_2, ag, taps, tfin, gsend, gown, grecv, tg_ref, tu_ref,
    loc, osem, xsem, ws, w0r, w1r, w2r, w3r, w4r, p1s, p1r, p2s, p2r, p3s, p3r,
    a1s, a1r, a2s, a2r, a3s, a3r, tss, tsr, gss, gsr,
):
    rep, y, c = lax.axis_index("rep"), lax.axis_index("fs"), lax.axis_index("tp")
    z, x = rep // 4, lax.rem(rep, 4)
    first, second = (x, z), (z, x)
    bufs, twos = (buf0, buf1, buf2), (two0, two1, two2)
    outs3, ins3 = (out3_0, out3_1, out3_2), (in3_0, in3_1, in3_2)

    def dev(dx=0, dz=0, dy=0, dc=0):
        return (wrap(z + dz) * 4 + wrap(x + dx), wrap(y + dy), wrap(c + dc, 2))

    def first_dev(p, d):
        return dev(dx=d) if p == 0 else dev(dz=d)

    def second_dev(p, d):
        return dev(dz=d) if p == 0 else dev(dx=d)

    def remote(src, dst, send, recv, where):
        return pltpu.make_async_remote_copy(
            src_ref=src, dst_ref=dst, send_sem=send, recv_sem=recv, device_id=where, device_id_type=MESH
        )

    def send(src, dst, send_sem, recv_sem, where):
        remote(src, dst, send_sem, recv_sem, where).start()

    def received(place, sem):
        remote(place, place, sem, sem, dev(dc=1)).wait_recv()

    def sent(place, sem):
        remote(place, place, sem, sem, dev(dc=1)).wait_send()

    local = []

    def load(src, dst):
        copy = pltpu.make_async_copy(src, dst, loc.at[len(local)])
        copy.start()
        local.append(copy)
        return copy

    tap_loads = [load(tg_hbm, tg_ref), load(tu_hbm, tu_ref)]
    pre = []
    for at, width in SPLITS:
        cols = pl.ds(at, width)
        pre.append(
            [load(h.at[0, :, cols], v.at[pl.ds(PAD, LEN), cols]) for h, v in ((pg_hbm, pg), (pu_hbm, pu), (ct_hbm, ct))]
        )
    mine = pl.ds(mult(c * HALF, HALF), HALF)
    x_local = load(x_hbm.at[0], xs.at[mine])
    w_local = [load(h, wall.at[g, y]) for g, h in enumerate((wg_hbm, wu_hbm))]
    pg[0:PAD, :] = jnp.zeros((PAD, COLS), bf16)
    pu[0:PAD, :] = jnp.zeros((PAD, COLS), bf16)

    peers = [dev(dx=d) for d in (1, 2, 3)] + [dev(dz=d) for d in (1, 2, 3)]
    peers += [dev(dy=d) for d in (1, 2, 3)] + [dev(dc=1)]
    barrier = pltpu.get_barrier_semaphore()
    for peer in peers:
        pl.semaphore_signal(barrier, inc=1, device_id=peer, device_id_type=MESH)
    pl.semaphore_wait(barrier, len(peers))

    send(x_hbm.at[0], xs.at[mine], xsem.at[0], xsem.at[1], dev(dc=1))
    ways = ((-1, x, 0, 512 - 4 * STRIPE), (1, z, 256, 0))

    def ring_dev(way, d):
        return dev(dx=d) if way == 0 else dev(dz=d)

    def stripe(way, d):
        source, at, _, base = ways[way]
        return wrap(y + source), pl.ds(mult(base + wrap(at + d) * STRIPE, STRIPE), STRIPE)

    def passed(way):
        source, _, start, _ = ways[way]
        return wrap(y + source), pl.ds(start, 256)

    def rest(way):
        source = ways[way][0]
        return wrap(y + source), pl.ds(256 if way == 0 else 4 * STRIPE, 256 - 4 * STRIPE)

    for level, rows_of in enumerate((lambda way: stripe(way, 0), passed, rest)):
        for g, h in enumerate((wg_hbm, wu_hbm)):
            for way in range(2):
                rows = rows_of(way)[1]
                sem = w0r.at[way] if level == 0 else w1r.at[way * 2 + level - 1]
                send(h.at[rows], wall.at[g, y, rows], ws.at[0], sem, dev(dy=-ways[way][0]))

    def stripe_start():
        for way in range(2):
            shard, rows = stripe(way, 0)
            place = wall.at[:, shard, rows]
            received(place, w0r.at[way])
            for side, d in enumerate((1, -1)):
                send(place, place, ws.at[1], w3r.at[way * 2 + side], ring_dev(way, d))

    def stripe_pass():
        for way in range(2):
            for side, d in enumerate((1, -1)):
                shard, rows = stripe(way, -d)
                received(wall.at[:, shard, rows], w3r.at[way * 2 + side])
                place = wall.at[side, shard, rows]
                send(place, place, ws.at[2], w4r.at[way * 2 + side], ring_dev(way, d))

    def stripe_end():
        for way in range(2):
            shard, rows = stripe(way, 2)
            for side in range(2):
                received(wall.at[side, shard, rows], w4r.at[way * 2 + side])

    def w_arrived(way, level):
        shard, rows = (passed, rest)[level](way)
        received(wall.at[:, shard, rows], w1r.at[way * 2 + level])

    def w_forward(piece):
        at, count = FAR[piece]
        for way in range(2):
            place = wall.at[:, wrap(y + ways[way][0]), pl.ds(way * 256 + at, count)]
            send(place, place, ws.at[3], w2r.at[way * len(FAR) + piece], dev(dy=-ways[way][0]))

    def w_far_arrived(piece):
        at, count = FAR[piece]
        for way in range(2):
            received(wall.at[:, wrap(y + 2), pl.ds(way * 256 + at, count)], w2r.at[way * len(FAR) + piece])

    def elementwise(k, low, high):
        at = SPLITS[k][0]

        def column(b, _):
            col = mult(at + b * 128, 128)
            cols = pl.ds(col, 128)
            shared = pl.ds(mult(c * COLS + col, 128), 128)
            kg = tg_ref[:, shared].astype(f32)
            ku = tu_ref[:, shared].astype(f32)
            kg = [kg[j : j + 1] for j in range(3)]
            ku = [ku[j : j + 1] for j in range(3)]

            def rows(i, carry):
                next_g, next_u, sums = carry
                r = mult(LEN - CHUNK - i * CHUNK, CHUNK)
                span, here = pl.ds(r, CHUNK + PAD), pl.ds(r + PAD, CHUNK)
                eg = pg[span, cols].astype(f32)[8:]
                eu = pu[span, cols].astype(f32)[8:]
                co = ct[here, cols].astype(f32)
                sg = [pltpu.roll(eg, 2, 0)[8:], pltpu.roll(eg, 1, 0)[8:], eg[8:]]
                su = [pltpu.roll(eu, 2, 0)[8:], pltpu.roll(eu, 1, 0)[8:], eu[8:]]
                v = kg[0] * sg[0] + kg[1] * sg[1] + kg[2] * sg[2]
                m = ku[0] * su[0] + ku[1] * su[1] + ku[2] * su[2]
                v2 = v * v
                t = jnp.tanh(v * (ROOT + (ROOT * CUBIC) * v2))
                h = 0.5 + 0.5 * t
                slope = h * (1.0 + v * (1.0 - t) * (ROOT + (3.0 * ROOT * CUBIC) * v2))
                bg = co * m * slope
                bu = co * (v * h)
                new = tuple(
                    s + (back * moved).reshape(CHUNK // 8, 8, 128).sum(0)
                    for s, (back, moved) in zip(sums, [(bg, q) for q in sg] + [(bu, q) for q in su])
                )
                for ref, back, after, taps_of in ((pg, bg, next_g, kg), (pu, bu, next_u, ku)):
                    whole = jnp.concatenate([back, after], axis=0)
                    one = pltpu.roll(whole, CHUNK + 7, 0)[:CHUNK]
                    two = pltpu.roll(whole, CHUNK + 6, 0)[:CHUNK]
                    ref[here, cols] = (taps_of[2] * back + taps_of[1] * one + taps_of[0] * two).astype(bf16)
                return bg[:8], bu[:8], new

            zero = jnp.zeros((8, 128), f32)
            _, _, sums = lax.fori_loop(0, LEN // CHUNK, rows, (zero, zero, (zero,) * 6))
            rows8 = [jnp.sum(s, axis=0, keepdims=True) for s in sums]
            taps[0, x, :, cols] = jnp.concatenate(rows8 + [jnp.zeros((2, 128), f32)], axis=0)
            return 0

        lax.fori_loop(low, high, column, 0)

    grads = (pg, pu)

    def own_rows(p, s):
        parts = []
        for yb in range(4):
            chunk = wrap(first[p] - 1 - s) if yb < 2 else wrap(first[p] + 1 + s)
            parts.append(xt[pl.ds(mult(yb * 512 + chunk * 128, 128), 128), :])
        return jnp.concatenate(parts, axis=0)

    def product(p, k, s):
        at, width = SPLITS[k]
        right = grads[p][PAD : PAD + LEN, at : at + width]
        return jnp.dot(own_rows(p, s), right, preferred_element_type=f32).reshape(4, 128, width)

    def p1_send(k, p, s):
        for way in range(2):
            pair = pl.ds(way * 2, 2)
            send(
                bufs[k].at[p, s, pair], bufs[k].at[p, s + 1, pair], p1s.at[k], p1r.at[(k * 2 + p) * 3 + s],
                first_dev(p, 1 - 2 * way),
            )

    def step0(k):
        for p in range(2):
            bufs[k][p, 0] = product(p, k, 0).astype(bf16)
            p1_send(k, p, 0)

    def step1(k, s):
        at, width = SPLITS[k]
        for p in range(2):
            own[p, :, :, 0:width] = product(p, k, s)
        for p in range(2):
            received(bufs[k].at[p, s], p1r.at[(k * 2 + p) * 3 + s - 1])

            def add(yb, _):
                total = bufs[k][p, s, yb].astype(f32) + own[p, yb, :, 0:width]
                if s < 3:
                    bufs[k][p, s, yb] = total.astype(bf16)
                else:
                    acc1[p, yb, :, at : at + width] = total
                return 0

            lax.fori_loop(0, 4, add, 0)
            if s < 3:
                p1_send(k, p, s)

    def p2_send(k, p, s):
        for way in range(2):
            pair = pl.ds(way * 2, 2)
            send(
                twos[k].at[p, s, pair], twos[k].at[p, s + 1, pair], p2s.at[k], p2r.at[(k * 2 + p) * 3 + s],
                second_dev(p, 1 - 2 * way),
            )

    def step2(k, s):
        at, width = SPLITS[k]
        for p in range(2):
            if s > 0:
                received(twos[k].at[p, s], p2r.at[(k * 2 + p) * 3 + s - 1])

            def add(yb, _):
                move = (1 - 2 * (yb // 2)) * (1 + s)
                chunk = wrap(second[p] - move)
                total = acc1[p, yb, pl.ds(mult(chunk * 32, 32), 32), at : at + width]
                if s > 0:
                    total = total + twos[k][p, s, yb].astype(f32)
                if s < 3:
                    twos[k][p, s, yb] = total.astype(bf16)
                else:
                    acc2[p, yb, :, at : at + width] = total
                return 0

            lax.fori_loop(0, 4, add, 0)
            if s < 3:
                p2_send(k, p, s)

    def p3_send(k):
        at, width = SPLITS[k]
        for p in range(2):
            for d in (1, 3, 2):
                outs3[k][p, d - 1] = acc2[p, wrap(y + d), :, at : at + width].astype(bf16)
                send(
                    outs3[k].at[p, d - 1], ins3[k].at[p, d - 1], p3s.at[k], p3r.at[k], dev(dy=d)
                )

    def block(p, group, d_first, d_second, skip=0, rows=32):
        start = wrap(first[p] + d_first) * 128 + wrap(second[p] + d_second) * 32 + skip
        at, width = GROUPS[group]
        return ag.at[p, pl.ds(mult(start, 16), rows), pl.ds(at, width)]

    def amount(group, rows):
        at, width = GROUPS[group]
        return ag.at[:, pl.ds(0, rows), pl.ds(at, width)]

    def p3_wait(k):
        received(ins3[k], p3r.at[k])

    def p3_finish(k, p):
        at, width = SPLITS[k]
        total = acc2[p, y, :, at : at + width]
        for d in (1, 3, 2):
            total = total + ins3[k][p, d - 1].astype(f32)
        start = mult(first[p] * 128 + second[p] * 32, 32)
        ag[p, pl.ds(start, 32), at : at + width] = total.astype(bf16)

    def a1_start(group, p):
        for d in (1, 3, 2):
            place = block(p, group, 0, 0)
            send(place, place, a1s.at[0], a1r.at[group * 3 + d - 1], second_dev(p, d))

    def a1_wait(group, d):
        received(amount(group, 32), a1r.at[group * 3 + d - 1])

    def a2_start(group, p, d):
        place = block(p, group, 0, -d)
        for way in range(2):
            send(place, place, a2s.at[0], a2r.at[group * 4 + d], first_dev(p, 1 - 2 * way))

    def a2_pass_on(group, d):
        received(amount(group, 64), a2r.at[group * 4 + d])
        for p in range(2):
            for way in range(2):
                from_ = 2 * way - 1
                part = block(p, group, from_, -d, 16 * way, 16)
                send(part, part, a3s.at[0], a3r.at[group], first_dev(p, -from_))

    def a3_wait(group):
        received(amount(group, 128), a3r.at[group])
        rows_out(group, 2)

    def rows_out(group, d):
        at, width = GROUPS[group]
        for p in range(2):
            part = p, pl.ds(mult(wrap(first[p] + d) * 128, 128), 128), pl.ds(at, width)
            pltpu.make_async_copy(ag.at[part], ag_out.at[part], osem.at[1]).start()

    def gather_start(group):
        p3_wait(group)
        for p in range(2):
            p3_finish(group, p)
            a1_start(group, p)
            a2_start(group, p, 0)

    def gather_second(group):
        for d in (1, 3, 2):
            a1_wait(group, d)
            for p in range(2):
                a2_start(group, p, d)

    coords = (x, z, y)

    def tap_dev(stage, d):
        return dev(dx=d) if stage == 0 else dev(dz=d) if stage == 1 else dev(dy=d)

    def tap_send(stage):
        place = taps.at[stage, coords[stage], 0:6]
        for d in (1, 2, 3):
            send(place, place, tss.at[stage], tsr.at[stage], tap_dev(stage, d))

    def tap_sum(stage):
        received(taps.at[stage, 0:3, 0:6], tsr.at[stage])
        total = taps[stage, 0] + taps[stage, 1] + taps[stage, 2] + taps[stage, 3]
        if stage < 2:
            taps[stage + 1, coords[stage + 1]] = total
            tap_send(stage + 1)
        else:
            tfin[c] = total * (float(TOKENS) ** -0.5)
            send(tfin.at[c], tfin.at[c], tss.at[3], tsr.at[3], dev(dc=1))

    def tap_end():
        other = tfin.at[wrap(c + 1, 2)]
        received(other, tsr.at[3])
        pltpu.make_async_copy(tfin, tap_out, osem.at[2]).start()

    def project(unit, d, starts):
        shard = wrap(y + d)

        def weights(g):
            return jnp.concatenate([wall[g, shard, at : at + 128, :] for at in starts], axis=0)

        def side(which, _):
            to_partner = 1 - which
            row = mult(PAD + wrap(c + to_partner, 2) * HALF, 16)
            dims = (((1,), (1,)), ((), ()))
            value = lax.dot_general(pg[pl.ds(row, HALF), :], weights(0), dims, preferred_element_type=f32)
            value = value + lax.dot_general(pu[pl.ds(row, HALF), :], weights(1), dims, preferred_element_type=f32)
            gsend[which, unit] = value.astype(bf16)
            return 0

        lax.fori_loop(0, 2, side, 0)
        send(gsend.at[0, unit], grecv.at[unit], gss.at[0], gsr.at[unit], dev(dc=1))

    def combine(unit, d, starts):
        received(grecv.at[unit], gsr.at[unit])
        gown[unit] = (gsend[1, unit].astype(f32) + grecv[unit].astype(f32)).astype(bf16)
        for i, at in enumerate(starts):
            col = mult(wrap(y + d) * 512 + at, 128)
            part = gown.at[unit, :, pl.ds(i * 128, 128)]
            pltpu.make_async_copy(part, gi_out.at[:, pl.ds(col, 128)], osem.at[0]).start()

    def turn_half(side, count, block_of):
        rows = pl.ds(mult(side * HALF, HALF), HALF)

        def turn(i, _):
            at = pl.ds(mult(block_of(i) * 128, 128), 128)
            xt[at, rows] = xs[rows, at].T
            return 0

        lax.fori_loop(0, count, turn, 0)

    def early(i):
        yb = lax.rem(i, 4)
        base = jnp.where(i < 4, x, z)
        return yb * 4 + wrap(base - 1 + 2 * (yb // 2))

    def late(i):
        yb = i // 3
        return yb * 4 + wrap(x + lax.rem(i, 3) + 2 * (yb // 2))

    for copy in tap_loads + pre[0]:
        copy.wait()
    elementwise(0, 0, 2)
    x_local.wait()
    turn_half(c, 8, early)
    other_half = xs.at[pl.ds(mult(wrap(c + 1, 2) * HALF, HALF), HALF)]
    received(other_half, xsem.at[1])
    turn_half(wrap(c + 1, 2), 8, early)
    units = [(0, (0, 128)), (0, (256, 384)), (-1, (0, 128)), (1, (256, 384)), (-1, (256, 384)), (1, (0, 128))]
    units += [(2, (0, 256)), (2, (128, 384))]
    step0(0)
    for copy in pre[1]:
        copy.wait()
    elementwise(1, 0, 2)
    stripe_start()
    elementwise(1, 2, 4)
    step0(1)
    turn_half(0, 12, late)
    turn_half(1, 12, late)
    step1(0, 1)
    for copy in pre[2]:
        copy.wait()
    elementwise(2, 0, 2)
    stripe_pass()
    elementwise(2, 2, 5)
    step0(2)
    step1(1, 1)
    step1(0, 2)
    for copy in w_local:
        copy.wait()
    project(0, *units[0])
    project(1, *units[1])
    step1(2, 1)
    step1(1, 2)
    for way in range(2):
        w_arrived(way, 0)
    w_forward(0)
    project(2, *units[2])
    step1(0, 3)
    step2(0, 0)
    project(3, *units[3])
    step1(2, 2)
    combine(0, *units[0])
    combine(1, *units[1])
    step1(1, 3)
    step2(1, 0)
    step2(0, 1)
    stripe_end()
    for way in range(2):
        w_arrived(way, 1)
    project(4, *units[4])
    combine(2, *units[2])
    combine(3, *units[3])
    step1(2, 3)
    step2(2, 0)
    w_forward(1)
    step2(1, 1)
    step2(0, 2)
    step2(2, 1)
    step2(1, 2)
    step2(0, 3)
    p3_send(0)
    step2(2, 2)
    step2(1, 3)
    p3_send(1)
    step2(2, 3)
    p3_send(2)
    tap_send(0)
    w_forward(2)
    w_forward(3)
    gather_start(0)
    project(5, *units[5])
    gather_start(1)
    gather_second(0)
    gather_start(2)
    tap_sum(0)
    w_far_arrived(0)
    gather_second(1)
    project(6, *units[6])
    gather_second(2)
    tap_sum(1)
    combine(4, *units[4])
    combine(5, *units[5])
    for group in range(3):
        for d in (0, 1, 3, 2):
            a2_pass_on(group, d)
        for d in (0, -1, 1):
            rows_out(group, d)
    for piece in range(1, len(FAR)):
        w_far_arrived(piece)
    tap_sum(2)
    project(7, *units[7])
    combine(6, *units[6])
    for group in range(3):
        a3_wait(group)
    tap_end()
    sent(xs.at[mine], xsem.at[0])
    sent(wall.at[:, 0:2, 0 : 512 - 3 * STRIPE], ws.at[0])
    sent(wall.at[:, 0, 0 : 4 * STRIPE], ws.at[1])
    sent(wall.at[0, 0, 0 : 4 * STRIPE], ws.at[2])
    sent(wall.at[:, 0], ws.at[3])
    for k in range(len(SPLITS)):
        sent(bufs[k].at[:, 0:3], p1s.at[k])
        sent(twos[k].at[:, 0:3], p2s.at[k])
        sent(outs3[k], p3s.at[k])
    for sem, rows in ((a1s, 96), (a2s, 256), (a3s, 128)):
        sent(ag.at[:, 0:rows], sem.at[0])
    for stage in range(3):
        sent(taps.at[stage, 0:3, 0:6], tss.at[stage])
    sent(tfin.at[0], tss.at[3])
    sent(gsend.at[0], gss.at[0])
    combine(7, *units[7])
    for sem, ref in enumerate((gown, ag, tfin)):
        pltpu.make_async_copy(ref, ref, osem.at[sem]).wait()


def finish(gi_in, ag_in, tap_in, gi_out, gate_out, up_out, tap_gate, tap_up, gi, half, full, tap, tg, tu, sems):
    copies, count = [], 8
    rows = 512 // count

    def start(src, dst):
        copy = pltpu.make_async_copy(src, dst, sems.at[len(copies)])
        copy.start()
        copies.append(copy)
        return copy

    gi_load = start(gi_in, gi)
    loads = []
    for i in range(count):
        part = pl.ds(i * rows, rows)
        loads.append(start(ag_in.at[:, part], half.at[:, part]))
    tap_load = start(tap_in, tap)
    gi_load.wait()
    stores = [start(gi, gi_out.at[0])]
    for i in range(count):
        part = pl.ds(i * rows, rows)
        loads[i].wait()
        for p, target in enumerate((gate_out, up_out)):
            full[p, part] = half[p, part].astype(f32) * (float(TOKENS) ** -0.5)
            stores.append(start(full.at[p, part], target.at[part]))
        if i == count // 2:
            tap_load.wait()
            for side in range(2):
                cols = slice(side * COLS, side * COLS + COLS)
                tg[:, cols] = tap[side, 0:3]
                tu[:, cols] = tap[side, 3:6]
            stores += [start(tg, tap_gate), start(tu, tap_up)]
    for copy in stores:
        copy.wait()


def per_device(inputs, pre_gate, pre_up, cotangent, w_gate, w_up, taps_gate, taps_up):
    any_ = pl.BlockSpec(memory_space=pl.ANY)
    dma = pltpu.SemaphoreType.DMA
    widths = [width for _, width in SPLITS]
    count = len(widths)
    scratch = (
        [pltpu.VMEM((PAD + LEN, COLS), bf16)] * 3
        + [pltpu.VMEM((LEN, WIDTH), bf16), pltpu.VMEM((WIDTH, LEN), bf16), pltpu.VMEM((2, 4, 512, COLS), bf16)]
        + [pltpu.VMEM((2, 4, 4, 128, width), bf16) for width in widths]
        + [pltpu.VMEM((2, 4, 128, max(widths)), f32), pltpu.VMEM((2, 4, 128, COLS), f32)]
        + [pltpu.VMEM((2, 4, 4, 32, width), bf16) for width in widths]
        + [pltpu.VMEM((2, 4, 32, COLS), f32)]
        + [pltpu.VMEM((2, 3, 32, width), bf16) for width in widths] * 2
        + [pltpu.VMEM((2, 512, COLS), bf16), pltpu.VMEM((3, 4, 8, COLS), f32), pltpu.VMEM((2, 8, COLS), f32)]
        + [pltpu.VMEM((2, 8, HALF, 256), bf16), pltpu.VMEM((8, HALF, 256), bf16), pltpu.VMEM((8, HALF, 256), bf16)]
        + [pltpu.VMEM((3, 2 * COLS), bf16)] * 2
        + [dma((14,)), dma((3,)), dma((2,)), dma((4,)), dma((2,)), dma((4,)), dma((2 * len(FAR),)), dma((4,)), dma((4,))]
        + [dma((count,)), dma((6 * count,))] * 2
        + [dma((count,)), dma((count,))]
        + [dma((1,)), dma((9,)), dma((1,)), dma((12,)), dma((1,)), dma((3,)), dma((4,)), dma((4,)), dma((1,)), dma((8,))]
    )
    grad_inputs, sums, tap_sums = pl.pallas_call(
        kernel,
        out_shape=(
            jax.ShapeDtypeStruct((HALF, WIDTH), bf16),
            jax.ShapeDtypeStruct((2, 512, COLS), bf16),
            jax.ShapeDtypeStruct((2, 8, COLS), f32),
        ),
        in_specs=[any_] * 8,
        out_specs=(any_,) * 3,
        scratch_shapes=scratch,
        compiler_params=pltpu.CompilerParams(
            collective_id=0, has_side_effects=True, vmem_limit_bytes=67043328
        ),
    )(inputs, pre_gate, pre_up, cotangent, w_gate, w_up, taps_gate, taps_up)
    return tuple(
        pl.pallas_call(
            finish,
            out_shape=(
                jax.ShapeDtypeStruct((1, HALF, WIDTH), bf16),
                jax.ShapeDtypeStruct((512, COLS), f32),
                jax.ShapeDtypeStruct((512, COLS), f32),
                jax.ShapeDtypeStruct((3, 2 * COLS), f32),
                jax.ShapeDtypeStruct((3, 2 * COLS), f32),
            ),
            in_specs=[any_] * 3,
            out_specs=(any_,) * 5,
            scratch_shapes=[
                pltpu.VMEM((HALF, WIDTH), bf16),
                pltpu.VMEM((2, 512, COLS), bf16),
                pltpu.VMEM((2, 512, COLS), f32),
                pltpu.VMEM((2, 8, COLS), f32),
                pltpu.VMEM((3, 2 * COLS), f32),
                pltpu.VMEM((3, 2 * COLS), f32),
                dma((32,)),
            ],
            compiler_params=pltpu.CompilerParams(vmem_limit_bytes=67043328),
        )(grad_inputs, sums, tap_sums)
    )


def solution(mesh):
    placed = (
        P(("rep", "fs"), "tp", None),
        P(("rep", "fs"), None, "tp"),
        P(("rep", "fs"), None, "tp"),
        P(("rep", "fs"), None, "tp"),
        P("fs", "tp"),
        P("fs", "tp"),
        P(),
        P(),
    )
    return jax.shard_map(
        per_device,
        mesh=mesh,
        in_specs=placed,
        out_specs=(P(("rep", "fs"), "tp", None), P("fs", "tp"), P("fs", "tp"), P(), P()),
        check_vma=False,
    )
```

```python
import functools

import jax
import jax.numpy as jnp
from jax import lax
from jax.experimental import pallas as pl
from jax.experimental.pallas import tpu as pltpu
from jax.sharding import PartitionSpec as P

MESH = pl.DeviceIdType.MESH
LEN = 768
COLS = 1408
WIDTH = 2048
TOKENS = 49152
SPLITS = ((0, 384), (384, 512), (896, 512))
CHUNK = 64
PAD = 16
STRIPE = 32
FAR = ((0, 128), (128, 32), (160, 32), (192, 64))
GROUPS = SPLITS
HALF = LEN // 2
ROOT = 0.7978845608028654
CUBIC = 0.044715
bf16, f32 = jnp.bfloat16, jnp.float32


def wrap(value, n=4):
    return lax.rem(value + 2 * n, n)


def mult(value, n):
    return pl.multiple_of(value, n)


def kernel(
    x_hbm, pg_hbm, pu_hbm, ct_hbm, wg_hbm, wu_hbm, tg_hbm, tu_hbm,
    gi_out, ag_out, tap_out,
    pg, pu, ct, xs, xt, wall, buf0, buf1, buf2, own, acc1, two0, two1, two2, acc2,
    out3_0, out3_1, out3_2, in3_0, in3_1, in3_2, ag, taps, tfin, gsend, gown, grecv, tg_ref, tu_ref,
    loc, osem, xsem, ws, w0r, w1r, w2r, w3r, w4r, p1s, p1r, p2s, p2r, p3s, p3r,
    a1s, a1r, a2s, a2r, a3s, a3r, tss, tsr, gss, gsr,
):
    rep, y, c = lax.axis_index("rep"), lax.axis_index("fs"), lax.axis_index("tp")
    z, x = rep // 4, lax.rem(rep, 4)
    first, second = (x, z), (z, x)
    bufs, twos = (buf0, buf1, buf2), (two0, two1, two2)
    outs3, ins3 = (out3_0, out3_1, out3_2), (in3_0, in3_1, in3_2)

    def dev(dx=0, dz=0, dy=0, dc=0):
        return (wrap(z + dz) * 4 + wrap(x + dx), wrap(y + dy), wrap(c + dc, 2))

    def first_dev(p, d):
        return dev(dx=d) if p == 0 else dev(dz=d)

    def second_dev(p, d):
        return dev(dz=d) if p == 0 else dev(dx=d)

    def remote(src, dst, send, recv, where):
        return pltpu.make_async_remote_copy(
            src_ref=src, dst_ref=dst, send_sem=send, recv_sem=recv, device_id=where, device_id_type=MESH
        )

    def send(src, dst, send_sem, recv_sem, where):
        remote(src, dst, send_sem, recv_sem, where).start()

    def received(place, sem):
        remote(place, place, sem, sem, dev(dc=1)).wait_recv()

    def sent(place, sem):
        remote(place, place, sem, sem, dev(dc=1)).wait_send()

    local = []

    def load(src, dst):
        copy = pltpu.make_async_copy(src, dst, loc.at[len(local)])
        copy.start()
        local.append(copy)
        return copy

    tap_loads = [load(tg_hbm, tg_ref), load(tu_hbm, tu_ref)]
    pre = []
    for at, width in SPLITS:
        cols = pl.ds(at, width)
        pre.append(
            [load(h.at[0, :, cols], v.at[pl.ds(PAD, LEN), cols]) for h, v in ((pg_hbm, pg), (pu_hbm, pu), (ct_hbm, ct))]
        )
    mine = pl.ds(mult(c * HALF, HALF), HALF)
    x_local = load(x_hbm.at[0], xs.at[mine])
    w_local = [load(h, wall.at[g, y]) for g, h in enumerate((wg_hbm, wu_hbm))]
    pg[0:PAD, :] = jnp.zeros((PAD, COLS), bf16)
    pu[0:PAD, :] = jnp.zeros((PAD, COLS), bf16)

    peers = [dev(dx=d) for d in (1, 2, 3)] + [dev(dz=d) for d in (1, 2, 3)]
    peers += [dev(dy=d) for d in (1, 2, 3)] + [dev(dc=1)]
    barrier = pltpu.get_barrier_semaphore()
    for peer in peers:
        pl.semaphore_signal(barrier, inc=1, device_id=peer, device_id_type=MESH)
    pl.semaphore_wait(barrier, len(peers))

    send(x_hbm.at[0], xs.at[mine], xsem.at[0], xsem.at[1], dev(dc=1))
    ways = ((-1, x, 0, 512 - 4 * STRIPE), (1, z, 256, 0))

    def ring_dev(way, d):
        return dev(dx=d) if way == 0 else dev(dz=d)

    def stripe(way, d):
        source, at, _, base = ways[way]
        return wrap(y + source), pl.ds(mult(base + wrap(at + d) * STRIPE, STRIPE), STRIPE)

    def passed(way):
        source, _, start, _ = ways[way]
        return wrap(y + source), pl.ds(start, 256)

    def rest(way):
        source = ways[way][0]
        return wrap(y + source), pl.ds(256 if way == 0 else 4 * STRIPE, 256 - 4 * STRIPE)

    for level, rows_of in enumerate((lambda way: stripe(way, 0), passed, rest)):
        for g, h in enumerate((wg_hbm, wu_hbm)):
            for way in range(2):
                rows = rows_of(way)[1]
                sem = w0r.at[way] if level == 0 else w1r.at[way * 2 + level - 1]
                send(h.at[rows], wall.at[g, y, rows], ws.at[0], sem, dev(dy=-ways[way][0]))

    def stripe_start():
        for way in range(2):
            shard, rows = stripe(way, 0)
            place = wall.at[:, shard, rows]
            received(place, w0r.at[way])
            for side, d in enumerate((1, -1)):
                send(place, place, ws.at[1], w3r.at[way * 2 + side], ring_dev(way, d))

    def stripe_pass():
        for way in range(2):
            for side, d in enumerate((1, -1)):
                shard, rows = stripe(way, -d)
                received(wall.at[:, shard, rows], w3r.at[way * 2 + side])
                place = wall.at[side, shard, rows]
                send(place, place, ws.at[2], w4r.at[way * 2 + side], ring_dev(way, d))

    def stripe_end():
        for way in range(2):
            shard, rows = stripe(way, 2)
            for side in range(2):
                received(wall.at[side, shard, rows], w4r.at[way * 2 + side])

    def w_arrived(way, level):
        shard, rows = (passed, rest)[level](way)
        received(wall.at[:, shard, rows], w1r.at[way * 2 + level])

    def w_forward(piece):
        at, count = FAR[piece]
        for way in range(2):
            place = wall.at[:, wrap(y + ways[way][0]), pl.ds(way * 256 + at, count)]
            send(place, place, ws.at[3], w2r.at[way * len(FAR) + piece], dev(dy=-ways[way][0]))

    def w_far_arrived(piece):
        at, count = FAR[piece]
        for way in range(2):
            received(wall.at[:, wrap(y + 2), pl.ds(way * 256 + at, count)], w2r.at[way * len(FAR) + piece])

    def elementwise(k, low, high):
        at = SPLITS[k][0]

        def column(b, _):
            col = mult(at + b * 128, 128)
            cols = pl.ds(col, 128)
            shared = pl.ds(mult(c * COLS + col, 128), 128)
            kg = tg_ref[:, shared].astype(f32)
            ku = tu_ref[:, shared].astype(f32)
            kg = [kg[j : j + 1] for j in range(3)]
            ku = [ku[j : j + 1] for j in range(3)]

            def rows(i, carry):
                next_g, next_u, sums = carry
                r = mult(LEN - CHUNK - i * CHUNK, CHUNK)
                span, here = pl.ds(r, CHUNK + PAD), pl.ds(r + PAD, CHUNK)
                eg = pg[span, cols].astype(f32)[8:]
                eu = pu[span, cols].astype(f32)[8:]
                co = ct[here, cols].astype(f32)
                sg = [pltpu.roll(eg, 2, 0)[8:], pltpu.roll(eg, 1, 0)[8:], eg[8:]]
                su = [pltpu.roll(eu, 2, 0)[8:], pltpu.roll(eu, 1, 0)[8:], eu[8:]]
                v = kg[0] * sg[0] + kg[1] * sg[1] + kg[2] * sg[2]
                m = ku[0] * su[0] + ku[1] * su[1] + ku[2] * su[2]
                v2 = v * v
                t = jnp.tanh(v * (ROOT + (ROOT * CUBIC) * v2))
                h = 0.5 + 0.5 * t
                slope = h * (1.0 + v * (1.0 - t) * (ROOT + (3.0 * ROOT * CUBIC) * v2))
                bg = co * m * slope
                bu = co * (v * h)
                new = tuple(
                    s + (back * moved).reshape(CHUNK // 8, 8, 128).sum(0)
                    for s, (back, moved) in zip(sums, [(bg, q) for q in sg] + [(bu, q) for q in su])
                )
                for ref, back, after, taps_of in ((pg, bg, next_g, kg), (pu, bu, next_u, ku)):
                    whole = jnp.concatenate([back, after], axis=0)
                    one = pltpu.roll(whole, CHUNK + 7, 0)[:CHUNK]
                    two = pltpu.roll(whole, CHUNK + 6, 0)[:CHUNK]
                    ref[here, cols] = (taps_of[2] * back + taps_of[1] * one + taps_of[0] * two).astype(bf16)
                return bg[:8], bu[:8], new

            zero = jnp.zeros((8, 128), f32)
            _, _, sums = lax.fori_loop(0, LEN // CHUNK, rows, (zero, zero, (zero,) * 6))
            rows8 = [jnp.sum(s, axis=0, keepdims=True) for s in sums]
            taps[0, x, :, cols] = jnp.concatenate(rows8 + [jnp.zeros((2, 128), f32)], axis=0)
            return 0

        lax.fori_loop(low, high, column, 0)

    grads = (pg, pu)

    def own_rows(p, s):
        parts = []
        for yb in range(4):
            chunk = wrap(first[p] - 1 - s) if yb < 2 else wrap(first[p] + 1 + s)
            parts.append(xt[pl.ds(mult(yb * 512 + chunk * 128, 128), 128), :])
        return jnp.concatenate(parts, axis=0)

    def product(p, k, s):
        at, width = SPLITS[k]
        right = grads[p][PAD : PAD + LEN, at : at + width]
        return jnp.dot(own_rows(p, s), right, preferred_element_type=f32).reshape(4, 128, width)

    def p1_send(k, p, s):
        for way in range(2):
            pair = pl.ds(way * 2, 2)
            send(
                bufs[k].at[p, s, pair], bufs[k].at[p, s + 1, pair], p1s.at[k], p1r.at[(k * 2 + p) * 3 + s],
                first_dev(p, 1 - 2 * way),
            )

    def step0(k):
        for p in range(2):
            bufs[k][p, 0] = product(p, k, 0).astype(bf16)
            p1_send(k, p, 0)

    def step1(k, s):
        at, width = SPLITS[k]
        for p in range(2):
            own[p, :, :, 0:width] = product(p, k, s)
        for p in range(2):
            received(bufs[k].at[p, s], p1r.at[(k * 2 + p) * 3 + s - 1])

            def add(yb, _):
                total = bufs[k][p, s, yb].astype(f32) + own[p, yb, :, 0:width]
                if s < 3:
                    bufs[k][p, s, yb] = total.astype(bf16)
                else:
                    acc1[p, yb, :, at : at + width] = total
                return 0

            lax.fori_loop(0, 4, add, 0)
            if s < 3:
                p1_send(k, p, s)

    def p2_send(k, p, s):
        for way in range(2):
            pair = pl.ds(way * 2, 2)
            send(
                twos[k].at[p, s, pair], twos[k].at[p, s + 1, pair], p2s.at[k], p2r.at[(k * 2 + p) * 3 + s],
                second_dev(p, 1 - 2 * way),
            )

    def step2(k, s):
        at, width = SPLITS[k]
        for p in range(2):
            if s > 0:
                received(twos[k].at[p, s], p2r.at[(k * 2 + p) * 3 + s - 1])

            def add(yb, _):
                move = (1 - 2 * (yb // 2)) * (1 + s)
                chunk = wrap(second[p] - move)
                total = acc1[p, yb, pl.ds(mult(chunk * 32, 32), 32), at : at + width]
                if s > 0:
                    total = total + twos[k][p, s, yb].astype(f32)
                if s < 3:
                    twos[k][p, s, yb] = total.astype(bf16)
                else:
                    acc2[p, yb, :, at : at + width] = total
                return 0

            lax.fori_loop(0, 4, add, 0)
            if s < 3:
                p2_send(k, p, s)

    def p3_send(k):
        at, width = SPLITS[k]
        for p in range(2):
            for d in (1, 3, 2):
                outs3[k][p, d - 1] = acc2[p, wrap(y + d), :, at : at + width].astype(bf16)
                send(
                    outs3[k].at[p, d - 1], ins3[k].at[p, d - 1], p3s.at[k], p3r.at[k], dev(dy=d)
                )

    def block(p, group, d_first, d_second, skip=0, rows=32):
        start = wrap(first[p] + d_first) * 128 + wrap(second[p] + d_second) * 32 + skip
        at, width = GROUPS[group]
        return ag.at[p, pl.ds(mult(start, 16), rows), pl.ds(at, width)]

    def amount(group, rows):
        at, width = GROUPS[group]
        return ag.at[:, pl.ds(0, rows), pl.ds(at, width)]

    def p3_wait(k):
        received(ins3[k], p3r.at[k])

    def p3_finish(k, p):
        at, width = SPLITS[k]
        total = acc2[p, y, :, at : at + width]
        for d in (1, 3, 2):
            total = total + ins3[k][p, d - 1].astype(f32)
        start = mult(first[p] * 128 + second[p] * 32, 32)
        ag[p, pl.ds(start, 32), at : at + width] = total.astype(bf16)

    def a1_start(group, p):
        for d in (1, 3, 2):
            place = block(p, group, 0, 0)
            send(place, place, a1s.at[0], a1r.at[group * 3 + d - 1], second_dev(p, d))

    def a1_wait(group, d):
        received(amount(group, 32), a1r.at[group * 3 + d - 1])

    def a2_start(group, p, d):
        place = block(p, group, 0, -d)
        for way in range(2):
            send(place, place, a2s.at[0], a2r.at[group * 4 + d], first_dev(p, 1 - 2 * way))

    def a2_pass_on(group, d):
        received(amount(group, 64), a2r.at[group * 4 + d])
        for p in range(2):
            for way in range(2):
                from_ = 2 * way - 1
                part = block(p, group, from_, -d, 16 * way, 16)
                send(part, part, a3s.at[0], a3r.at[group], first_dev(p, -from_))

    def a3_wait(group):
        received(amount(group, 128), a3r.at[group])
        rows_out(group, 2)

    def rows_out(group, d):
        at, width = GROUPS[group]
        for p in range(2):
            part = p, pl.ds(mult(wrap(first[p] + d) * 128, 128), 128), pl.ds(at, width)
            pltpu.make_async_copy(ag.at[part], ag_out.at[part], osem.at[1]).start()

    def gather_start(group):
        p3_wait(group)
        for p in range(2):
            p3_finish(group, p)
            a1_start(group, p)
            a2_start(group, p, 0)

    def gather_second(group):
        for d in (1, 3, 2):
            a1_wait(group, d)
            for p in range(2):
                a2_start(group, p, d)

    coords = (x, z, y)

    def tap_dev(stage, d):
        return dev(dx=d) if stage == 0 else dev(dz=d) if stage == 1 else dev(dy=d)

    def tap_send(stage):
        place = taps.at[stage, coords[stage], 0:6]
        for d in (1, 2, 3):
            send(place, place, tss.at[stage], tsr.at[stage], tap_dev(stage, d))

    def tap_sum(stage):
        received(taps.at[stage, 0:3, 0:6], tsr.at[stage])
        total = taps[stage, 0] + taps[stage, 1] + taps[stage, 2] + taps[stage, 3]
        if stage < 2:
            taps[stage + 1, coords[stage + 1]] = total
            tap_send(stage + 1)
        else:
            tfin[c] = total * (float(TOKENS) ** -0.5)
            send(tfin.at[c], tfin.at[c], tss.at[3], tsr.at[3], dev(dc=1))

    def tap_end():
        other = tfin.at[wrap(c + 1, 2)]
        received(other, tsr.at[3])
        pltpu.make_async_copy(tfin, tap_out, osem.at[2]).start()

    def project(unit, d, starts):
        shard = wrap(y + d)

        def weights(g):
            return jnp.concatenate([wall[g, shard, at : at + 128, :] for at in starts], axis=0)

        def side(which, _):
            to_partner = 1 - which
            row = mult(PAD + wrap(c + to_partner, 2) * HALF, 16)
            dims = (((1,), (1,)), ((), ()))
            value = lax.dot_general(pg[pl.ds(row, HALF), :], weights(0), dims, preferred_element_type=f32)
            value = value + lax.dot_general(pu[pl.ds(row, HALF), :], weights(1), dims, preferred_element_type=f32)
            gsend[which, unit] = value.astype(bf16)
            return 0

        lax.fori_loop(0, 2, side, 0)
        send(gsend.at[0, unit], grecv.at[unit], gss.at[0], gsr.at[unit], dev(dc=1))

    def combine(unit, d, starts):
        received(grecv.at[unit], gsr.at[unit])
        gown[unit] = (gsend[1, unit].astype(f32) + grecv[unit].astype(f32)).astype(bf16)
        for i, at in enumerate(starts):
            col = mult(wrap(y + d) * 512 + at, 128)
            part = gown.at[unit, :, pl.ds(i * 128, 128)]
            pltpu.make_async_copy(part, gi_out.at[:, pl.ds(col, 128)], osem.at[0]).start()

    def turn_half(side, count, block_of):
        rows = pl.ds(mult(side * HALF, HALF), HALF)

        def turn(i, _):
            at = pl.ds(mult(block_of(i) * 128, 128), 128)
            xt[at, rows] = xs[rows, at].T
            return 0

        lax.fori_loop(0, count, turn, 0)

    def early(i):
        yb = lax.rem(i, 4)
        base = jnp.where(i < 4, x, z)
        return yb * 4 + wrap(base - 1 + 2 * (yb // 2))

    def late(i):
        yb = i // 3
        return yb * 4 + wrap(x + lax.rem(i, 3) + 2 * (yb // 2))

    for copy in tap_loads + pre[0]:
        copy.wait()
    elementwise(0, 0, 3)
    x_local.wait()
    turn_half(c, 8, early)
    other_half = xs.at[pl.ds(mult(wrap(c + 1, 2) * HALF, HALF), HALF)]
    received(other_half, xsem.at[1])
    turn_half(wrap(c + 1, 2), 8, early)
    units = [(0, (0, 128)), (0, (256, 384)), (-1, (0, 128)), (1, (256, 384)), (-1, (256, 384)), (1, (0, 128))]
    units += [(2, (0, 256)), (2, (128, 384))]
    step0(0)
    for copy in pre[1]:
        copy.wait()
    elementwise(1, 0, 1)
    stripe_start()
    elementwise(1, 1, 4)
    step0(1)
    turn_half(0, 12, late)
    turn_half(1, 12, late)
    step1(0, 1)
    for copy in pre[2]:
        copy.wait()
    elementwise(2, 0, 2)
    stripe_pass()
    elementwise(2, 2, 4)
    step0(2)
    step1(1, 1)
    step1(0, 2)
    for copy in w_local:
        copy.wait()
    project(0, *units[0])
    project(1, *units[1])
    step1(2, 1)
    step1(1, 2)
    for way in range(2):
        w_arrived(way, 0)
    w_forward(0)
    project(2, *units[2])
    step1(0, 3)
    step2(0, 0)
    project(3, *units[3])
    step1(2, 2)
    combine(0, *units[0])
    combine(1, *units[1])
    step1(1, 3)
    step2(1, 0)
    step2(0, 1)
    stripe_end()
    for way in range(2):
        w_arrived(way, 1)
    project(4, *units[4])
    combine(2, *units[2])
    combine(3, *units[3])
    step1(2, 3)
    step2(2, 0)
    w_forward(1)
    step2(1, 1)
    step2(0, 2)
    step2(2, 1)
    step2(1, 2)
    step2(0, 3)
    p3_send(0)
    step2(2, 2)
    step2(1, 3)
    p3_send(1)
    step2(2, 3)
    p3_send(2)
    tap_send(0)
    w_forward(2)
    w_forward(3)
    gather_start(0)
    project(5, *units[5])
    gather_start(1)
    gather_second(0)
    gather_start(2)
    tap_sum(0)
    w_far_arrived(0)
    gather_second(1)
    project(6, *units[6])
    gather_second(2)
    tap_sum(1)
    combine(4, *units[4])
    combine(5, *units[5])
    for group in range(3):
        for d in (0, 1, 3, 2):
            a2_pass_on(group, d)
        for d in (0, -1, 1):
            rows_out(group, d)
    for piece in range(1, len(FAR)):
        w_far_arrived(piece)
    tap_sum(2)
    project(7, *units[7])
    combine(6, *units[6])
    for group in range(3):
        a3_wait(group)
    tap_end()
    sent(xs.at[mine], xsem.at[0])
    sent(wall.at[:, 0:2, 0 : 512 - 3 * STRIPE], ws.at[0])
    sent(wall.at[:, 0, 0 : 4 * STRIPE], ws.at[1])
    sent(wall.at[0, 0, 0 : 4 * STRIPE], ws.at[2])
    sent(wall.at[:, 0], ws.at[3])
    for k in range(len(SPLITS)):
        sent(bufs[k].at[:, 0:3], p1s.at[k])
        sent(twos[k].at[:, 0:3], p2s.at[k])
        sent(outs3[k], p3s.at[k])
    for sem, rows in ((a1s, 96), (a2s, 256), (a3s, 128)):
        sent(ag.at[:, 0:rows], sem.at[0])
    for stage in range(3):
        sent(taps.at[stage, 0:3, 0:6], tss.at[stage])
    sent(tfin.at[0], tss.at[3])
    sent(gsend.at[0], gss.at[0])
    combine(7, *units[7])
    for sem, ref in enumerate((gown, ag, tfin)):
        pltpu.make_async_copy(ref, ref, osem.at[sem]).wait()


def finish(gi_in, ag_in, tap_in, gi_out, gate_out, up_out, tap_gate, tap_up, gi, half, full, tap, tg, tu, sems):
    copies, count = [], 8
    rows = 512 // count

    def start(src, dst):
        copy = pltpu.make_async_copy(src, dst, sems.at[len(copies)])
        copy.start()
        copies.append(copy)
        return copy

    gi_load = start(gi_in, gi)
    loads = []
    for i in range(count):
        part = pl.ds(i * rows, rows)
        loads.append(start(ag_in.at[:, part], half.at[:, part]))
    tap_load = start(tap_in, tap)
    gi_load.wait()
    stores = [start(gi, gi_out.at[0])]
    for i in range(count):
        part = pl.ds(i * rows, rows)
        loads[i].wait()
        for p, target in enumerate((gate_out, up_out)):
            full[p, part] = half[p, part].astype(f32) * (float(TOKENS) ** -0.5)
            stores.append(start(full.at[p, part], target.at[part]))
        if i == count // 2:
            tap_load.wait()
            for side in range(2):
                cols = slice(side * COLS, side * COLS + COLS)
                tg[:, cols] = tap[side, 0:3]
                tu[:, cols] = tap[side, 3:6]
            stores += [start(tg, tap_gate), start(tu, tap_up)]
    for copy in stores:
        copy.wait()


def per_device(inputs, pre_gate, pre_up, cotangent, w_gate, w_up, taps_gate, taps_up):
    any_ = pl.BlockSpec(memory_space=pl.ANY)
    dma = pltpu.SemaphoreType.DMA
    widths = [width for _, width in SPLITS]
    count = len(widths)
    scratch = (
        [pltpu.VMEM((PAD + LEN, COLS), bf16)] * 3
        + [pltpu.VMEM((LEN, WIDTH), bf16), pltpu.VMEM((WIDTH, LEN), bf16), pltpu.VMEM((2, 4, 512, COLS), bf16)]
        + [pltpu.VMEM((2, 4, 4, 128, width), bf16) for width in widths]
        + [pltpu.VMEM((2, 4, 128, max(widths)), f32), pltpu.VMEM((2, 4, 128, COLS), f32)]
        + [pltpu.VMEM((2, 4, 4, 32, width), bf16) for width in widths]
        + [pltpu.VMEM((2, 4, 32, COLS), f32)]
        + [pltpu.VMEM((2, 3, 32, width), bf16) for width in widths] * 2
        + [pltpu.VMEM((2, 512, COLS), bf16), pltpu.VMEM((3, 4, 8, COLS), f32), pltpu.VMEM((2, 8, COLS), f32)]
        + [pltpu.VMEM((2, 8, HALF, 256), bf16), pltpu.VMEM((8, HALF, 256), bf16), pltpu.VMEM((8, HALF, 256), bf16)]
        + [pltpu.VMEM((3, 2 * COLS), bf16)] * 2
        + [dma((14,)), dma((3,)), dma((2,)), dma((4,)), dma((2,)), dma((4,)), dma((2 * len(FAR),)), dma((4,)), dma((4,))]
        + [dma((count,)), dma((6 * count,))] * 2
        + [dma((count,)), dma((count,))]
        + [dma((1,)), dma((9,)), dma((1,)), dma((12,)), dma((1,)), dma((3,)), dma((4,)), dma((4,)), dma((1,)), dma((8,))]
    )
    grad_inputs, sums, tap_sums = pl.pallas_call(
        kernel,
        out_shape=(
            jax.ShapeDtypeStruct((HALF, WIDTH), bf16),
            jax.ShapeDtypeStruct((2, 512, COLS), bf16),
            jax.ShapeDtypeStruct((2, 8, COLS), f32),
        ),
        in_specs=[any_] * 8,
        out_specs=(any_,) * 3,
        scratch_shapes=scratch,
        compiler_params=pltpu.CompilerParams(
            collective_id=0, has_side_effects=True, vmem_limit_bytes=67043328
        ),
    )(inputs, pre_gate, pre_up, cotangent, w_gate, w_up, taps_gate, taps_up)
    return tuple(
        pl.pallas_call(
            finish,
            out_shape=(
                jax.ShapeDtypeStruct((1, HALF, WIDTH), bf16),
                jax.ShapeDtypeStruct((512, COLS), f32),
                jax.ShapeDtypeStruct((512, COLS), f32),
                jax.ShapeDtypeStruct((3, 2 * COLS), f32),
                jax.ShapeDtypeStruct((3, 2 * COLS), f32),
            ),
            in_specs=[any_] * 3,
            out_specs=(any_,) * 5,
            scratch_shapes=[
                pltpu.VMEM((HALF, WIDTH), bf16),
                pltpu.VMEM((2, 512, COLS), bf16),
                pltpu.VMEM((2, 512, COLS), f32),
                pltpu.VMEM((2, 8, COLS), f32),
                pltpu.VMEM((3, 2 * COLS), f32),
                pltpu.VMEM((3, 2 * COLS), f32),
                dma((32,)),
            ],
            compiler_params=pltpu.CompilerParams(vmem_limit_bytes=67043328),
        )(grad_inputs, sums, tap_sums)
    )


def solution(mesh):
    placed = (
        P(("rep", "fs"), "tp", None),
        P(("rep", "fs"), None, "tp"),
        P(("rep", "fs"), None, "tp"),
        P(("rep", "fs"), None, "tp"),
        P("fs", "tp"),
        P("fs", "tp"),
        P(),
        P(),
    )
    return jax.shard_map(
        per_device,
        mesh=mesh,
        in_specs=placed,
        out_specs=(P(("rep", "fs"), "tp", None), P("fs", "tp"), P("fs", "tp"), P(), P()),
        check_vma=False,
    )
```
